512 devices in a mesh: sp: 128 (over z, x, core), tp: 4 (over y).
Axes of the slice: x: 4, y: 4, z: 16, core: 2. Of those that a mesh axis runs over, the one named last changes fastest.
Arguments:
- tokens: bfloat16 [16384, 2048], P(('sp', 'tp')), may hold values from -6 to 6
- norm_gain: float32 [2048], replicated, may hold values from 0.1 to 1.9
- w_query: bfloat16 [2048, 512], P(None, 'tp'), may hold values from -0.125 to 0.125
- w_key: bfloat16 [2048, 512], P(None, 'tp'), may hold values from -0.125 to 0.125
- w_value: bfloat16 [2048, 512], P(None, 'tp'), may hold values from -0.125 to 0.125
- score_offset: float32 [8], P('tp'), may hold values from -13 to -3, as said below
- w_out: bfloat16 [512, 2048], P('tp'), may hold values from -0.25 to 0.25
Outputs:
- mixed: bfloat16 [16384, 2048], P(('sp', 'tp'))
The draws below stay inside these ranges and needn't reach their ends.
Inputs may be any that keep to these rules, and one draw needn't show every extreme that they name: `score_offset`: one offset a head.
All inputs are finite; a program needn't handle non-finite values.
Results may differ from the reference program's by a relative error of at most 0.01.
Values may be sent and summed in bfloat16 or wider, within the bound.
A program may use at most 64 MiB of HBM per device.

```python
import math
import jax
import jax.numpy as jnp
from jax import lax

D = 2048
HEADS = 8
HEAD_DIM = 64
SEQ = 16384
WIDTH = 512
N_TP = 4


def draw_score_offset(key, part):
    key_slow, key_fast, key_pick = jax.random.split(jax.random.fold_in(key, 7), 3)
    slow_level = -jnp.log(jnp.float32(SEQ)) + jax.random.uniform(key_slow, (HEADS,), jnp.float32, -0.5, 0.5)
    fast_level = jax.random.uniform(key_fast, (HEADS,), jnp.float32, -4.5, -3.0)
    ranks = jax.random.permutation(key_pick, HEADS)
    slow_heads = ranks < HEADS // 2
    return jnp.where(slow_heads, slow_level, fast_level).astype(jnp.float32)


def shard_levels(key, extent, cuts, smallest, high):
    gain, own = 1.0, jax.random.fold_in(key, 6)
    for position, parts in cuts:
        steps = jnp.exp(jax.random.uniform(jax.random.fold_in(own, position), (parts,), jnp.float32, smallest / len(cuts), high / len(cuts)))
        gain = gain * jnp.repeat(steps, extent[position] // parts).reshape([-1 if axis == position else 1 for axis in range(len(extent))])
    return gain


def centred(rng, extent, spread, bound, pieces=(), kind=jnp.bfloat16):
    result = spread * jax.random.normal(rng, extent, jnp.float32)
    if pieces:
        result = result * shard_levels(rng, extent, pieces, -0.22, 0.18)
    return jnp.clip(result, -bound, bound).astype(kind)


def setup_inputs(seed: int = 0) -> dict:
    key_of = jax.random.split(jax.random.key(seed), 8)
    return {
        "tokens": centred(key_of[0], (SEQ, D), 1.0, 6.0, ((0, 512),)),
        "norm_gain": jnp.clip(1.0 + 0.18 * jax.random.normal(key_of[1], (D,), jnp.float32), 0.1, 1.9),
        "w_query": centred(key_of[2], (D, WIDTH), D ** -0.5, 0.125, ((1, 4),)),
        "w_key": centred(key_of[3], (D, WIDTH), D ** -0.5, 0.125, ((1, 4),)),
        "w_value": centred(key_of[4], (D, WIDTH), D ** -0.5, 0.125, ((1, 4),)),
        "score_offset": draw_score_offset(jax.random.fold_in(key_of[7], 71), 0),
        "w_out": centred(key_of[6], (WIDTH, D), WIDTH ** -0.5, 0.25, ((0, 4),)),
    }


RMS_EPS = 1e-06

def reference(tokens, norm_gain, w_query, w_key, w_value, score_offset, w_out):
    rows_f32 = tokens.astype(jnp.float32)
    inv_rms = lax.rsqrt(lax.optimization_barrier(jnp.mean(rows_f32 * rows_f32, axis=1, keepdims=True)) + RMS_EPS)
    normed = (rows_f32 * inv_rms * norm_gain.astype(jnp.float32)).astype(jnp.bfloat16)
    queries = jnp.dot(normed, w_query, preferred_element_type=jnp.float32).astype(jnp.bfloat16)
    keys = jnp.dot(normed, w_key, preferred_element_type=jnp.float32).astype(jnp.bfloat16)
    values = jnp.dot(normed, w_value, preferred_element_type=jnp.float32).astype(jnp.bfloat16)
    query_heads = queries.reshape(SEQ, HEADS, HEAD_DIM).transpose(1, 0, 2)
    key_heads = keys.reshape(SEQ, HEADS, HEAD_DIM).transpose(1, 0, 2)
    value_heads = values.reshape(SEQ, HEADS, HEAD_DIM).transpose(1, 0, 2)
    block_rows = math.gcd(SEQ, 512)
    blocks = SEQ // block_rows
    key_pos = jnp.arange(SEQ, dtype=jnp.int32)

    def head_fn(args):
        query_part, key_part, value_part, offset = args

        def block_fn(index):
            start = (index * block_rows).astype(jnp.int32)
            query_rows = lax.dynamic_slice_in_dim(query_part, start, block_rows, 0)
            scores = jnp.dot(query_rows, key_part.T, preferred_element_type=jnp.float32) * HEAD_DIM ** (-0.5) + offset
            query_pos = start + jnp.arange(block_rows, dtype=jnp.int32)
            earlier = key_pos[None, :] < query_pos[:, None]
            log_keep = jnp.where(earlier, jax.nn.log_sigmoid(-scores), 0.0)
            suffix = lax.cumsum(log_keep, axis=1, reverse=True) - log_keep
            weights = jnp.where(earlier, jnp.exp(jax.nn.log_sigmoid(scores) + suffix), 0.0).astype(jnp.bfloat16)
            return jnp.dot(weights, value_part, preferred_element_type=jnp.float32).astype(jnp.bfloat16)
        return lax.map(block_fn, jnp.arange(blocks, dtype=jnp.int32)).reshape(SEQ, HEAD_DIM)
    attended = lax.map(head_fn, (query_heads, key_heads, value_heads, score_offset.astype(jnp.float32)))
    group = HEADS // N_TP
    grouped = attended.reshape(N_TP, group, SEQ, HEAD_DIM).transpose(0, 2, 1, 3).reshape(N_TP, SEQ, group * HEAD_DIM)
    weight_groups = w_out.reshape(N_TP, group * HEAD_DIM, D)

    def partial_fn(args):
        rows, weight = args
        rounded = jnp.dot(rows, weight, preferred_element_type=jnp.float32).astype(jnp.bfloat16)
        return lax.optimization_barrier(rounded).astype(jnp.float32)
    partials = lax.map(partial_fn, (grouped, weight_groups))
    return lax.optimization_barrier(jnp.sum(partials, axis=0)).astype(jnp.bfloat16)
```

```python
import functools

import jax
import jax.numpy as jnp
from jax import lax
from jax.experimental import pallas as pl
from jax.experimental.pallas import tpu as pltpu
from jax.sharding import PartitionSpec as P

HEAD_DIM = 64
RMS_EPS = 1e-06
LOG2E = 1.4426950408889634
MESH = pl.DeviceIdType.MESH
NT = (((1,), (1,)), ((), ()))
NEG = -1e30
F32 = jnp.float32
BF16 = jnp.bfloat16


def dot(a, b):
    return jnp.dot(a, b, preferred_element_type=F32)


def layer_kernel(
    tok_ref, gain_ref, off_ref, wq_hbm, wk_hbm, wv_hbm, wo_hbm, out_ref,
    wq, wk, wv, wo_all, tok_all, normed, sib_out, sib_in, q_out, q_in, q_pad,
    kv_all, vt_all, z_s, l_s, part_o, part_s, o_out, s_out, o_in, s_in, acc_o, acc_s,
    att_out, att_in,
    sem_w, ysend, yrecv, y2send, y2recv, bsend, brecv, qsend, qrecv,
    zsend, zrecv, xsend, xrecv, x2send, x2recv, osend, orecv, ssend, srecv,
    wsend, wrecv, w2send, w2recv, asend, arecv,
):
    sp = lax.axis_index("sp")
    y = lax.axis_index("tp")
    z = sp // 8
    x = (sp // 2) % 4
    c = sp % 2
    group = z // 4
    r = z % 4

    def at(z_, x_, c_, y_):
        return ((z_ * 4 + x_) * 2 + c_, y_)

    def remote(src, dst, ss, rs, dev):
        return pltpu.make_async_remote_copy(
            src_ref=src, dst_ref=dst, send_sem=ss, recv_sem=rs, device_id=dev, device_id_type=MESH
        )

    loads = [
        pltpu.make_async_copy(wq_hbm, wq, sem_w.at[0]),
        pltpu.make_async_copy(wk_hbm, wk, sem_w.at[1]),
        pltpu.make_async_copy(wv_hbm, wv, sem_w.at[2]),
        pltpu.make_async_copy(wo_hbm, wo_all.at[y], sem_w.at[3]),
    ]
    for cp in loads:
        cp.start()

    y_up, y_dn, y_far = (y + 1) % 4, (y + 3) % 4, (y + 2) % 4
    peers = (at(z, x, c, y_up), at(z, x, c, y_dn))
    first = {}
    for h, d in ((0, 0), (1, 1), (1, 0), (0, 1)):
        cp = remote(tok_ref.at[h], tok_all.at[y, h], ysend.at[d, h], yrecv.at[d, h], peers[d])
        cp.start()
        first[d, h] = cp

    gain = gain_ref[...]

    def norm_rows(rows):
        rows = rows.astype(F32)
        inv = lax.rsqrt(jnp.mean(rows * rows, axis=1, keepdims=True) + RMS_EPS)
        return (rows * inv * gain).astype(BF16)

    for h in range(2):
        normed[y, pl.ds(h * 16, 16), :] = norm_rows(tok_ref[h])

    row_i = lax.broadcasted_iota(jnp.int32, (256, 256), 0)
    col_i = lax.broadcasted_iota(jnp.int32, (256, 256), 1)
    perm = jnp.where((row_i % 8) * 32 + row_i // 8 == col_i, 1.0, 0.0).astype(BF16)

    first[0, 0].wait_recv()
    relay0 = remote(tok_all.at[y_dn, 0], tok_all.at[y_dn, 0], y2send.at[0], y2recv.at[0], peers[0])
    relay0.start()
    first[1, 1].wait_recv()
    relay1 = remote(tok_all.at[y_up, 1], tok_all.at[y_up, 1], y2send.at[1], y2recv.at[1], peers[1])
    relay1.start()
    normed[y_dn, pl.ds(0, 16), :] = norm_rows(tok_all[y_dn, 0])
    normed[y_up, pl.ds(16, 16), :] = norm_rows(tok_all[y_up, 1])
    first[0, 1].wait_recv()
    normed[y_dn, pl.ds(16, 16), :] = norm_rows(tok_all[y_dn, 1])
    first[1, 0].wait_recv()
    normed[y_up, pl.ds(0, 16), :] = norm_rows(tok_all[y_up, 0])
    for cp in loads:
        cp.wait()
    relay0.wait_recv()
    normed[y_far, pl.ds(0, 16), :] = norm_rows(tok_all[y_far, 0])
    relay1.wait_recv()
    normed[y_far, pl.ds(16, 16), :] = norm_rows(tok_all[y_far, 1])

    rows = normed[...].reshape(128, 2048)
    q = dot(rows, wq[...])
    k = dot(rows, wk[...])
    v = dot(rows, wv[...])
    lane = lax.broadcasted_iota(jnp.int32, (128, 128), 1)
    low = lane < HEAD_DIM
    kv0 = jnp.where(low, k, pltpu.roll(v, HEAD_DIM, 1)).astype(BF16)
    kv1 = jnp.where(low, pltpu.roll(k, HEAD_DIM, 1), v).astype(BF16)
    mine0 = c == 0
    sib_out[0] = jnp.where(mine0, kv1, kv0)
    sib_out[1] = pltpu.roll(q, HEAD_DIM, 1).astype(BF16)
    sib = remote(sib_out, sib_in, bsend, brecv, at(z, x, 1 - c, y))
    sib.start()
    kv_mine = jnp.where(mine0, kv0, kv1)

    wo_sends = []
    for n, yy in enumerate((y_up, y_dn, y_far)):
        cp = remote(wo_all.at[y, c], wo_all.at[y, c], wsend.at[n], wrecv.at[n], at(z, x, c, yy))
        cp.start()
        wo_sends.append(cp)

    sib.wait_recv()
    q_first = (lane < HEAD_DIM) == mine0
    q_out[...] = jnp.where(q_first, q, sib_in[1].astype(F32)).astype(BF16)
    kv_sib = sib_in[0]
    pair = jnp.concatenate([jnp.where(mine0, kv_mine, kv_sib), jnp.where(mine0, kv_sib, kv_mine)], axis=0)
    kv_all[r, x] = dot(perm, pair).astype(BF16)

    def q_copy(n):
        return remote(q_out, q_in.at[n - 1], qsend.at[n - 1], qrecv.at[n - 1], at((z + 16 - 4 * n) % 16, x, c, y))

    def z_copy(n):
        return remote(
            kv_all.at[r, x], kv_all.at[r, x], zsend.at[n - 1], zrecv.at[n - 1],
            at(group * 4 + (r + n) % 4, x, c, y),
        )

    def x_copy(d, n):
        plane = (r + 4 - n) % 4
        return remote(
            kv_all.at[plane, x], kv_all.at[plane, x], xsend.at[d, n], xrecv.at[d, n],
            at(z, (x + (1 if d == 0 else 3)) % 4, c, y),
        )

    def x_relay(n):
        plane = (r + 4 - n) % 4
        d = 0 if n < 2 else 1
        src = (x + (3 if d == 0 else 1)) % 4
        return remote(
            kv_all.at[plane, src], kv_all.at[plane, src], x2send.at[n], x2recv.at[n],
            at(z, (x + (1 if d == 0 else 3)) % 4, c, y),
        )

    for n in (1, 3, 2):
        z_copy(n).start()
    for d in range(2):
        x_copy(d, 0).start()
    for n in (1, 2, 3):
        @pl.when(group >= n)
        def _():
            q_copy(n).start()

    def relay_step(n):
        d = 0 if n < 2 else 1
        x_copy(d, n).wait_recv()
        x_relay(n).start()

    def rest_step(n):
        d = 0 if n < 2 else 1
        x_copy(1 - d, n).wait_recv()
        x_relay(n).wait_recv()

    def pad_query(n, packed):
        packed = packed.astype(F32)
        q_pad[n, pl.ds(0, 128), :] = jnp.where(low, packed, 0.0).astype(BF16)
        q_pad[n, pl.ds(128, 128), :] = jnp.where(low, pltpu.roll(packed, HEAD_DIM, 1), 0.0).astype(BF16)

    pad_query(0, q_out[...])
    offset = off_ref[c] * LOG2E
    scale = HEAD_DIM ** (-0.5) * LOG2E
    sub = lax.broadcasted_iota(jnp.int32, (8, 256), 0)
    lane_q = lax.broadcasted_iota(jnp.int32, (32, 8, 256), 2)
    key_in = lax.broadcasted_iota(jnp.int32, (32, 8, 256), 1) * 32 + lax.broadcasted_iota(
        jnp.int32, (32, 8, 256), 0
    )

    def transpose_plane(plane):
        for b in range(4):
            vt_all[plane, :, pl.ds(b * 256, 256)] = (
                kv_all[plane, b].astype(F32).T[HEAD_DIM:, :].astype(BF16)
            )

    def item(n, plane, masked):
        qn = q_pad[n]
        sums = []
        for b in range(4):
            zz = lax.dot_general(kv_all[plane, b], qn, NT, preferred_element_type=F32)
            z2 = zz.reshape(32, 8, 256) * scale + offset
            if masked:
                z2 = jnp.where(key_in + b * 256 < lane_q + x * 256, z2, NEG)
            keep = jnp.maximum(z2, jnp.log2(1.0 + jnp.exp2(jnp.minimum(z2, 126.0))))
            z_s[b] = z2
            l_s[b] = keep
            sums.append(jnp.sum(keep, axis=0))
        later = jnp.zeros((1, 256), F32)
        for b in range(3, -1, -1):
            total = sums[b]
            incl = total
            for step in (1, 2, 4):
                moved = pltpu.roll(incl, 8 - step, 0)
                incl = incl + jnp.where(sub < 8 - step, moved, 0.0)
            run = incl - total + later
            later = later + incl[0:1]
            for i in range(31, -1, -1):
                run = run + l_s[b, i]
                z_s[b, i] = jnp.exp2(z_s[b, i] - run)
        w = z_s[...].reshape(1024, 256).astype(BF16)
        part_o[n, plane] = dot(vt_all[plane], w)
        part_s[n, plane] = jnp.broadcast_to(later, (8, 256))

    def blank(n, plane):
        part_o[n, plane] = jnp.zeros((HEAD_DIM, 256), F32)
        part_s[n, plane] = jnp.zeros((8, 256), F32)

    relay_step(0)
    for n in (1, 3, 2):
        z_copy(n).wait_recv()
        x_copy(0, n).start()
        x_copy(1, n).start()
    rest_step(0)
    transpose_plane(r)
    item(0, r, True)
    for n in (1, 3, 2):
        relay_step(n)
    for n in (1, 3, 2):
        rest_step(n)
        transpose_plane((r + 4 - n) % 4)

    def planes_of_own(n, _):
        plane = (r + 4 - n) % 4

        @pl.when(n <= r)
        def _():
            item(0, plane, False)

        @pl.when(n > r)
        def _():
            blank(0, plane)

        return 0

    lax.fori_loop(1, 4, planes_of_own, 0)

    def finish(n):
        o = part_o[n, 3]
        s = part_s[n, 3][0:1]
        for plane in (2, 1, 0):
            o = o + jnp.exp2(-s) * part_o[n, plane]
            s = s + part_s[n, plane][0:1]
        return o, s

    def o_copy(n):
        dev = at((z + 4 * n) % 16, x, c, y)
        return (
            remote(o_out.at[n - 1], o_in.at[n - 1], osend.at[n - 1], orecv.at[n - 1], dev),
            remote(s_out.at[n - 1], s_in.at[n - 1], ssend.at[n - 1], srecv.at[n - 1], dev),
        )

    for n in (3, 2, 1):
        @pl.when(group + n <= 3)
        def _():
            q_copy(n).wait_recv()
            pad_query(n, q_in[n - 1])

            def planes(plane, _):
                item(n, plane, False)
                return 0

            lax.fori_loop(0, 4, planes, 0)
            o, s = finish(n)
            o_out[n - 1] = o.astype(BF16)
            s_out[n - 1] = jnp.broadcast_to(s, (8, 256))
            for cp in o_copy(n):
                cp.start()

    wo_fwd = []
    for n, yy in enumerate((y_dn, y_up, y_far)):
        wo_sends[n].wait_recv()
        cp = remote(wo_all.at[yy, c], wo_all.at[yy, c], w2send.at[n], w2recv.at[n], at(z, x, 1 - c, y))
        cp.start()
        wo_fwd.append(cp)

    o, s = finish(0)
    acc_o[...] = o
    acc_s[...] = jnp.broadcast_to(s, (8, 256))
    for n in (1, 2, 3):
        @pl.when(group >= n)
        def _():
            for cp in o_copy(n):
                cp.wait_recv()
            s_ = acc_s[0:1, :]
            acc_o[...] += jnp.exp2(-s_) * o_in[n - 1].astype(F32)
            acc_s[...] += s_in[n - 1]

    o = acc_o[...]
    both = jnp.concatenate([jnp.where(mine0, o, 0.0), jnp.where(mine0, 0.0, o)], axis=0)
    att_out[...] = both.T.astype(BF16).reshape(8, 32, 128)
    a_sends = []
    for n in range(1, 8):
        cc = (c + n // 4) % 2
        yy = (y + n) % 4
        cp = remote(
            att_out.at[cc * 4 + yy], att_in.at[y * 2 + c], asend.at[n - 1], arecv.at[n - 1],
            at(z, x, cc, yy),
        )
        cp.start()
        a_sends.append(cp)
    att_in[y * 2 + c] = att_out[c * 4 + y]
    for cp in wo_fwd:
        cp.wait_recv()
    for cp in a_sends:
        cp.wait_recv()
    total = jnp.zeros((32, 2048), F32)
    for yy in range(4):
        feats = (att_in[2 * yy].astype(F32) + att_in[2 * yy + 1].astype(F32)).astype(BF16)
        part = dot(feats, wo_all[yy].reshape(128, 2048))
        total = total + part.astype(BF16).astype(F32)
    out_ref[...] = total.astype(BF16)

    for cp in first.values():
        cp.wait_send()
    relay0.wait_send()
    relay1.wait_send()
    sib.wait_send()
    for cp in wo_sends + wo_fwd + a_sends:
        cp.wait_send()
    for n in (1, 2, 3):
        z_copy(n).wait_send()

        @pl.when(group >= n)
        def _():
            q_copy(n).wait_send()

        @pl.when(group + n <= 3)
        def _():
            for cp in o_copy(n):
                cp.wait_send()

    for n in range(4):
        x_copy(0, n).wait_send()
        x_copy(1, n).wait_send()
        x_relay(n).wait_send()


def per_device(tokens, norm_gain, w_query, w_key, w_value, score_offset, w_out):
    vmem = pl.BlockSpec(memory_space=pltpu.VMEM)
    hbm = pl.BlockSpec(memory_space=pl.ANY)
    dma = pltpu.SemaphoreType.DMA
    v = pltpu.VMEM
    return pl.pallas_call(
        layer_kernel,
        out_shape=jax.ShapeDtypeStruct((32, 2048), BF16),
        in_specs=[vmem, vmem, pl.BlockSpec(memory_space=pltpu.SMEM), hbm, hbm, hbm, hbm],
        out_specs=vmem,
        scratch_shapes=[
            v((2048, 128), BF16), v((2048, 128), BF16), v((2048, 128), BF16), v((4, 2, 64, 2048), BF16),
            v((4, 2, 16, 2048), BF16), v((4, 32, 2048), BF16),
            v((2, 128, 128), BF16), v((2, 128, 128), BF16),
            v((128, 128), BF16), v((3, 128, 128), BF16), v((4, 256, 128), BF16),
            v((4, 4, 256, 128), BF16), v((4, HEAD_DIM, 1024), BF16),
            v((4, 32, 8, 256), F32), v((4, 32, 8, 256), F32),
            v((4, 4, HEAD_DIM, 256), F32), v((4, 4, 8, 256), F32),
            v((3, HEAD_DIM, 256), BF16), v((3, 8, 256), F32),
            v((3, HEAD_DIM, 256), BF16), v((3, 8, 256), F32),
            v((HEAD_DIM, 256), F32), v((8, 256), F32),
            v((8, 32, 128), BF16), v((8, 32, 128), BF16),
            dma((4,)), dma((2, 2)), dma((2, 2)), dma((2,)), dma((2,)), dma, dma, dma((3,)), dma((3,)),
            dma((3,)), dma((3,)), dma((2, 4)), dma((2, 4)), dma((4,)), dma((4,)),
            dma((3,)), dma((3,)), dma((3,)), dma((3,)),
            dma((3,)), dma((3,)), dma((3,)), dma((3,)), dma((7,)), dma((7,)),
        ],
        compiler_params=pltpu.CompilerParams(has_side_effects=True, vmem_limit_bytes=48 << 20),
    )(
        tokens.reshape(2, 16, 2048), norm_gain.reshape(1, 2048), score_offset,
        w_query, w_key, w_value, w_out.reshape(2, 64, 2048),
    )


def solution(mesh):
    rows = P(("sp", "tp"), None)
    placed = (rows, P(), P(None, "tp"), P(None, "tp"), P(None, "tp"), P("tp"), P("tp", None))
    return jax.shard_map(per_device, mesh=mesh, in_specs=placed, out_specs=rows, check_vma=False)
```

```python
import functools

import jax
import jax.numpy as jnp
from jax import lax
from jax.experimental import pallas as pl
from jax.experimental.pallas import tpu as pltpu
from jax.sharding import PartitionSpec as P

HEAD_DIM = 64
RMS_EPS = 1e-06
LOG2E = 1.4426950408889634
MESH = pl.DeviceIdType.MESH
NT = (((1,), (1,)), ((), ()))
NEG = -1e30
F32 = jnp.float32
BF16 = jnp.bfloat16


def dot(a, b):
    return jnp.dot(a, b, preferred_element_type=F32)


def layer_kernel(
    tok_hbm, gain_hbm, off_hbm, wq_hbm, wk_hbm, wv_hbm, wo_hbm, out_ref,
    tok_ref, gain_ref, off_ref, wq, wk, wv, wo_all, tok_all, normed, sib_out, sib_in, q_out, q_in, q_pad,
    kv_all, vt_all, e_s, l_s, w_s, part_o, part_s, o_out, s_out, o_in, s_in, acc_o, acc_s,
    att_out, att_in,
    sem_w, ysend, yrecv, y2send, y2recv, bsend, brecv, qsend, qrecv,
    zsend, zrecv, xsend, xrecv, x2send, x2recv, osend, orecv, ssend, srecv,
    wsend, wrecv, w2send, w2recv, asend, arecv, hello,
):
    sp = lax.axis_index("sp")
    y = lax.axis_index("tp")
    z = sp // 8
    x = (sp // 2) % 4
    c = sp % 2
    group = z // 4
    r = z % 4

    def at(z_, x_, c_, y_):
        return ((z_ * 4 + x_) * 2 + c_, y_)

    def remote(src, dst, ss, rs, dev):
        return pltpu.make_async_remote_copy(
            src_ref=src, dst_ref=dst, send_sem=ss, recv_sem=rs, device_id=dev, device_id_type=MESH
        )

    early = [
        pltpu.make_async_copy(tok_hbm, tok_ref, sem_w.at[4]),
        pltpu.make_async_copy(gain_hbm, gain_ref, sem_w.at[5]),
        pltpu.make_async_copy(off_hbm, off_ref, sem_w.at[6]),
    ]
    for cp in early:
        cp.start()
    loads = [
        pltpu.make_async_copy(wq_hbm, wq, sem_w.at[0]),
        pltpu.make_async_copy(wk_hbm, wk, sem_w.at[1]),
        pltpu.make_async_copy(wv_hbm, wv, sem_w.at[2]),
        pltpu.make_async_copy(wo_hbm, wo_all.at[y], sem_w.at[3]),
    ]
    for cp in loads:
        cp.start()

    y_up, y_dn, y_far = (y + 1) % 4, (y + 3) % 4, (y + 2) % 4
    peers = (at(z, x, c, y_up), at(z, x, c, y_dn))

    def greet(sem, devs):
        for dev in devs:
            pl.semaphore_signal(sem, inc=1, device_id=dev, device_id_type=MESH)
        pl.semaphore_wait(sem, len(devs))

    def along_z(n):
        return [at((z + n) % 16, x, c, y), at((z + 16 - n) % 16, x, c, y)]

    partner = at(z, x, 1 - c, y)
    sides = [at(z, (x + 1) % 4, c, y), at(z, (x + 3) % 4, c, y)]
    greet(pltpu.get_barrier_semaphore(), [*peers, partner, *sides, *along_z(1)])
    for cp in early:
        cp.wait()
    first = {}
    for h, d in ((0, 0), (1, 1), (1, 0), (0, 1)):
        cp = remote(tok_ref.at[h], tok_all.at[y, h], ysend.at[d, h], yrecv.at[d, h], peers[d])
        cp.start()
        first[d, h] = cp

    greet(hello.at[0], [*peers, partner, *along_z(1)])
    gain = gain_ref[...]

    def norm_rows(rows):
        rows = rows.astype(F32)
        inv = lax.rsqrt(jnp.mean(rows * rows, axis=1, keepdims=True) + RMS_EPS)
        return (rows * inv * gain).astype(BF16)

    for h in range(2):
        normed[y, pl.ds(h * 16, 16), :] = norm_rows(tok_ref[h])

    row_i = lax.broadcasted_iota(jnp.int32, (256, 256), 0)
    col_i = lax.broadcasted_iota(jnp.int32, (256, 256), 1)
    perm = jnp.where((row_i % 8) * 32 + row_i // 8 == col_i, 1.0, 0.0).astype(BF16)

    first[0, 0].wait_recv()
    relay0 = remote(tok_all.at[y_dn, 0], tok_all.at[y_dn, 0], y2send.at[0], y2recv.at[0], peers[0])
    relay0.start()
    first[1, 1].wait_recv()
    relay1 = remote(tok_all.at[y_up, 1], tok_all.at[y_up, 1], y2send.at[1], y2recv.at[1], peers[1])
    relay1.start()
    greet(hello.at[1], [partner, *along_z(2)])
    for dev in along_z(4):
        pl.semaphore_signal(hello.at[2], inc=1, device_id=dev, device_id_type=MESH)
    q_pad[...] = jnp.zeros((4, 256, 128), BF16)
    normed[y_dn, pl.ds(0, 16), :] = norm_rows(tok_all[y_dn, 0])
    normed[y_up, pl.ds(16, 16), :] = norm_rows(tok_all[y_up, 1])
    first[0, 1].wait_recv()
    normed[y_dn, pl.ds(16, 16), :] = norm_rows(tok_all[y_dn, 1])
    first[1, 0].wait_recv()
    normed[y_up, pl.ds(0, 16), :] = norm_rows(tok_all[y_up, 0])
    for cp in loads:
        cp.wait()
    relay0.wait_recv()
    normed[y_far, pl.ds(0, 16), :] = norm_rows(tok_all[y_far, 0])
    relay1.wait_recv()
    normed[y_far, pl.ds(16, 16), :] = norm_rows(tok_all[y_far, 1])

    rows = normed[...].reshape(128, 2048)
    q = dot(rows, wq[...])
    k = dot(rows, wk[...])
    v = dot(rows, wv[...])
    lane = lax.broadcasted_iota(jnp.int32, (128, 128), 1)
    low = lane < HEAD_DIM
    kv0 = jnp.where(low, k, pltpu.roll(v, HEAD_DIM, 1)).astype(BF16)
    kv1 = jnp.where(low, pltpu.roll(k, HEAD_DIM, 1), v).astype(BF16)
    mine0 = c == 0
    sib_out[0] = jnp.where(mine0, kv1, kv0)
    sib_out[1] = pltpu.roll(q, HEAD_DIM, 1).astype(BF16)
    sib = remote(sib_out, sib_in, bsend, brecv, at(z, x, 1 - c, y))
    sib.start()
    kv_mine = jnp.where(mine0, kv0, kv1)

    wo_sends = []
    for n, yy in enumerate((y_up, y_dn, y_far)):
        cp = remote(wo_all.at[y, c], wo_all.at[y, c], wsend.at[n], wrecv.at[n], at(z, x, c, yy))
        cp.start()
        wo_sends.append(cp)

    sib.wait_recv()
    q_first = (lane < HEAD_DIM) == mine0
    q_out[...] = jnp.where(q_first, q, sib_in[1].astype(F32)).astype(BF16)
    kv_sib = sib_in[0]
    pair = jnp.concatenate([jnp.where(mine0, kv_mine, kv_sib), jnp.where(mine0, kv_sib, kv_mine)], axis=0)
    kv_all[r, x] = dot(perm, pair).astype(BF16)

    pl.semaphore_wait(hello.at[2], 2)

    def q_copy(n):
        return remote(q_out, q_in.at[n - 1], qsend.at[n - 1], qrecv.at[n - 1], at((z + 16 - 4 * n) % 16, x, c, y))

    planes = (r, r + 1 - 2 * (r % 2), (r + 2) % 4, 3 - r)

    def z_copy(n):
        return remote(
            kv_all.at[r, x], kv_all.at[r, x], zsend.at[n - 1], zrecv.at[n - 1], at(group * 4 + planes[n], x, c, y)
        )

    def x_copy(d, n):
        block = kv_all.at[planes[n], x]
        return remote(block, block, xsend.at[d, n], xrecv.at[d, n], sides[d])

    def x_relay(n):
        d = 0 if n < 2 else 1
        block = kv_all.at[planes[n], (x + (3 if d == 0 else 1)) % 4]
        return remote(block, block, x2send.at[n], x2recv.at[n], sides[d])

    def spread(n):
        if n:
            z_copy(n).wait_recv()
        x_copy(0, n).start()
        x_copy(1, n).start()

    def forward(n):
        x_copy(0 if n < 2 else 1, n).wait_recv()
        x_relay(n).start()

    low_half = lane < HEAD_DIM

    def complete(n):
        x_copy(1 if n < 2 else 0, n).wait_recv()
        x_relay(n).wait_recv()
        for b in range(4):
            vt_all[planes[n], :, pl.ds(b * 256, 256)] = (
                kv_all[planes[n], b].astype(F32).T[HEAD_DIM:, :].astype(BF16)
            )

    def pad_query(n, packed):
        packed = packed.astype(F32)
        q_pad[n, pl.ds(0, 128), :] = jnp.where(low_half, packed, 0.0).astype(BF16)
        q_pad[n, pl.ds(128, 128), :] = jnp.where(low_half, pltpu.roll(packed, HEAD_DIM, 1), 0.0).astype(BF16)

    def arrive(n):
        @pl.when(group + n <= 3)
        def _():
            q_copy(n).wait_recv()
            pad_query(n, q_in[n - 1])

    offset = off_ref[c] * LOG2E
    scale = HEAD_DIM ** (-0.5) * LOG2E
    sub = lax.broadcasted_iota(jnp.int32, (8, 512), 0)
    ahead = lax.broadcasted_iota(jnp.int32, (8, 256), 0) * 32 - lax.broadcasted_iota(jnp.int32, (8, 256), 1)

    def block(first_n, plane):
        sums = []
        for b in range(4):
            total = [None, None]
            for h in range(2):
                lanes = pl.ds(h * 256, 256)
                zz = lax.dot_general(kv_all[plane, b], q_pad[first_n + h], NT, preferred_element_type=F32)
                zz = zz.reshape(32, 8, 256)
                limit = x * 256 - b * 256 + (r - plane) * 1024
                for g in range(31, -1, -2):
                    up = []
                    for i in (g, g - 1):
                        e = jnp.exp2(jnp.minimum(zz[i] * scale + offset, 60.0))
                        if first_n + h == 0:
                            e = jnp.where(ahead < limit - i, e, 0.0)
                        e_s[b, i, :, lanes] = e
                        up.append(1.0 + e)
                    keep = jnp.log2(up[0] * up[1])
                    l_s[b, g // 2, :, lanes] = keep
                    total[h] = keep if total[h] is None else total[h] + keep
            sums.append(jnp.concatenate(total, axis=1))
        later = jnp.zeros((1, 512), F32)
        for b in range(3, -1, -1):
            total = sums[b]
            incl = total
            for step in (1, 2, 4):
                moved = pltpu.roll(incl, 8 - step, 0)
                incl = incl + jnp.where(sub < 8 - step, moved, 0.0)
            run = incl - total + later
            later = later + incl[0:1]
            for g in range(31, -1, -2):
                run = run + l_s[b, g // 2]
                left = jnp.exp2(-run)
                e = e_s[b, g - 1]
                w_s[b, g // 2] = jnp.concatenate([e * left, e_s[b, g] * (left * (1.0 + e))], axis=0).astype(BF16)
        o = dot(vt_all[plane], w_s[...].reshape(1024, 512))
        for h in range(2):
            part_o[first_n + h, plane] = o[:, h * 256 : h * 256 + 256]
            part_s[first_n + h, plane] = jnp.broadcast_to(later[:, h * 256 : h * 256 + 256], (8, 256))

    def near(n):
        @pl.when(jnp.logical_or(group < 3, planes[n] <= r))
        def _():
            block(0, planes[n])

        @pl.when(jnp.logical_and(group == 3, planes[n] > r))
        def _():
            part_o[0, planes[n]] = jnp.zeros((HEAD_DIM, 256), F32)
            part_s[0, planes[n]] = jnp.zeros((8, 256), F32)

    def far(n):
        @pl.when(group < 2)
        def _():
            block(2, planes[n])

    def finish(n):
        o = part_o[n, 3]
        s = part_s[n, 3][0:1]
        for plane in (2, 1, 0):
            o = o + jnp.exp2(-s) * part_o[n, plane]
            s = s + part_s[n, plane][0:1]
        return o, s

    def o_copy(n):
        dev = at((z + 4 * n) % 16, x, c, y)
        return (
            remote(o_out.at[n - 1], o_in.at[n - 1], osend.at[n - 1], orecv.at[n - 1], dev),
            remote(s_out.at[n - 1], s_in.at[n - 1], ssend.at[n - 1], srecv.at[n - 1], dev),
        )

    def give_back(n):
        @pl.when(group + n <= 3)
        def _():
            o, s = finish(n)
            o_out[n - 1] = o.astype(BF16)
            s_out[n - 1] = jnp.broadcast_to(s, (8, 256))
            for cp in o_copy(n):
                cp.start()

    spread(0)
    z_copy(1).start()
    for n in (2, 1, 3):
        @pl.when(group >= n)
        def _():
            q_copy(n).start()
    z_copy(2).start()
    z_copy(3).start()
    pad_query(0, q_out[...])
    forward(0)
    spread(1)
    complete(0)
    spread(2)
    forward(1)
    arrive(1)
    near(0)
    spread(3)
    forward(2)
    complete(1)
    arrive(2)
    arrive(3)
    far(0)
    near(1)
    forward(3)
    complete(2)
    far(1)
    near(2)
    complete(3)
    far(2)
    far(3)
    give_back(2)
    give_back(3)
    near(3)
    give_back(1)

    wo_fwd = []
    for n, yy in enumerate((y_dn, y_up, y_far)):
        wo_sends[n].wait_recv()
        cp = remote(wo_all.at[yy, c], wo_all.at[yy, c], w2send.at[n], w2recv.at[n], at(z, x, 1 - c, y))
        cp.start()
        wo_fwd.append(cp)

    o, s = finish(0)
    acc_o[...] = o
    acc_s[...] = jnp.broadcast_to(s, (8, 256))
    for n in (1, 2, 3):
        @pl.when(group >= n)
        def _():
            for cp in o_copy(n):
                cp.wait_recv()
            s_ = acc_s[0:1, :]
            acc_o[...] += jnp.exp2(-s_) * o_in[n - 1].astype(F32)
            acc_s[...] += s_in[n - 1]

    o = acc_o[...]
    both = jnp.concatenate([jnp.where(mine0, o, 0.0), jnp.where(mine0, 0.0, o)], axis=0)
    att_out[...] = both.T.astype(BF16).reshape(8, 32, 128)
    a_sends = []
    for n in range(1, 8):
        cc = (c + n // 4) % 2
        yy = (y + n) % 4
        cp = remote(
            att_out.at[cc * 4 + yy], att_in.at[y * 2 + c], asend.at[n - 1], arecv.at[n - 1],
            at(z, x, cc, yy),
        )
        cp.start()
        a_sends.append(cp)
    att_in[y * 2 + c] = att_out[c * 4 + y]
    for cp in wo_fwd:
        cp.wait_recv()
    for cp in a_sends:
        cp.wait_recv()
    total = jnp.zeros((32, 2048), F32)
    for yy in range(4):
        feats = (att_in[2 * yy].astype(F32) + att_in[2 * yy + 1].astype(F32)).astype(BF16)
        part = dot(feats, wo_all[yy].reshape(128, 2048))
        total = total + part.astype(BF16).astype(F32)
    out_ref[...] = total.astype(BF16)

    for cp in first.values():
        cp.wait_send()
    relay0.wait_send()
    relay1.wait_send()
    sib.wait_send()
    for cp in wo_sends + wo_fwd + a_sends:
        cp.wait_send()
    for n in (1, 2, 3):
        z_copy(n).wait_send()

        @pl.when(group >= n)
        def _():
            q_copy(n).wait_send()

        @pl.when(group + n <= 3)
        def _():
            for cp in o_copy(n):
                cp.wait_send()

    for n in range(4):
        x_copy(0, n).wait_send()
        x_copy(1, n).wait_send()
        x_relay(n).wait_send()


def per_device(tokens, norm_gain, w_query, w_key, w_value, score_offset, w_out):
    hbm = pl.BlockSpec(memory_space=pl.ANY)
    dma = pltpu.SemaphoreType.DMA
    v = pltpu.VMEM
    return pl.pallas_call(
        layer_kernel,
        out_shape=jax.ShapeDtypeStruct((32, 2048), BF16),
        in_specs=[hbm] * 7,
        out_specs=pl.BlockSpec(memory_space=pltpu.VMEM),
        scratch_shapes=[
            v((2, 16, 2048), BF16), v((1, 2048), F32), pltpu.SMEM((2,), F32),
            v((2048, 128), BF16), v((2048, 128), BF16), v((2048, 128), BF16), v((4, 2, 64, 2048), BF16),
            v((4, 2, 16, 2048), BF16), v((4, 32, 2048), BF16),
            v((2, 128, 128), BF16), v((2, 128, 128), BF16),
            v((128, 128), BF16), v((3, 128, 128), BF16), v((4, 256, 128), BF16),
            v((4, 4, 256, 128), BF16), v((4, HEAD_DIM, 1024), BF16),
            v((4, 32, 8, 512), F32), v((4, 16, 8, 512), F32), v((4, 16, 16, 512), BF16),
            v((4, 4, HEAD_DIM, 256), F32), v((4, 4, 8, 256), F32),
            v((3, HEAD_DIM, 256), BF16), v((3, 8, 256), F32),
            v((3, HEAD_DIM, 256), BF16), v((3, 8, 256), F32),
            v((HEAD_DIM, 256), F32), v((8, 256), F32),
            v((8, 32, 128), BF16), v((8, 32, 128), BF16),
            dma((7,)), dma((2, 2)), dma((2, 2)), dma((2,)), dma((2,)), dma, dma, dma((3,)), dma((3,)),
            dma((3,)), dma((3,)), dma((2, 4)), dma((2, 4)), dma((4,)), dma((4,)),
            dma((3,)), dma((3,)), dma((3,)), dma((3,)),
            dma((3,)), dma((3,)), dma((3,)), dma((3,)), dma((7,)), dma((7,)), pltpu.SemaphoreType.REGULAR((3,)),
        ],
        compiler_params=pltpu.CompilerParams(has_side_effects=True, collective_id=0, vmem_limit_bytes=67043328),
    )(
        tokens.reshape(2, 16, 2048), norm_gain.reshape(1, 2048), score_offset,
        w_query, w_key, w_value, w_out.reshape(2, 64, 2048),
    )


def solution(mesh):
    rows = P(("sp", "tp"), None)
    placed = (rows, P(), P(None, "tp"), P(None, "tp"), P(None, "tp"), P("tp"), P("tp", None))
    return jax.shard_map(per_device, mesh=mesh, in_specs=placed, out_specs=rows, check_vma=False)
```

```python
import functools

import jax
import jax.numpy as jnp
from jax import lax
from jax.experimental import pallas as pl
from jax.experimental.pallas import tpu as pltpu
from jax.sharding import PartitionSpec as P

HEAD_DIM = 64
RMS_EPS = 1e-06
LOG2E = 1.4426950408889634
MESH = pl.DeviceIdType.MESH
NT = (((1,), (1,)), ((), ()))
NEG = -1e30
F32 = jnp.float32
BF16 = jnp.bfloat16


def dot(a, b):
    return jnp.dot(a, b, preferred_element_type=F32)


def layer_kernel(
    tok_hbm, gain_hbm, off_hbm, wq_hbm, wk_hbm, wv_hbm, wo_hbm, out_ref,
    tok_ref, gain_ref, off_ref, w_qkv, wo_all, tok_all, normed, sib_out, sib_in, q_out, q_in, q_pad,
    kv_all, vt_all, e_s, l_s, w_s, part_o, part_s, o_out, s_out, o_in, s_in, acc_o, acc_s,
    att_out, att_in,
    sem_w, ysend, yrecv, y2recv, bsend, brecv, qsend, qrecv,
    zsend, zrecv, xsend, xrecv, x2recv, osend, orecv, ssend, srecv,
    wsend, wrecv, w2send, w2recv, asend, arecv, hello,
):
    sp = lax.axis_index("sp")
    y = lax.axis_index("tp")
    z = sp // 8
    x = (sp // 2) % 4
    c = sp % 2
    group = z // 4
    r = z % 4

    def at(z_, x_, c_, y_):
        return ((z_ * 4 + x_) * 2 + c_, y_)

    def remote(src, dst, ss, rs, dev):
        return pltpu.make_async_remote_copy(
            src_ref=src, dst_ref=dst, send_sem=ss, recv_sem=rs, device_id=dev, device_id_type=MESH
        )

    def settle(ref, sem):
        pltpu.make_async_copy(ref, ref, sem).wait()

    early = [
        pltpu.make_async_copy(tok_hbm, tok_ref, sem_w.at[2]),
        pltpu.make_async_copy(gain_hbm, gain_ref, sem_w.at[3]),
        pltpu.make_async_copy(off_hbm, off_ref, sem_w.at[4]),
    ]
    for cp in early:
        cp.start()
    loads = [
        pltpu.make_async_copy(wq_hbm, w_qkv.at[0], sem_w.at[0]),
        pltpu.make_async_copy(wk_hbm, w_qkv.at[1], sem_w.at[0]),
        pltpu.make_async_copy(wv_hbm, w_qkv.at[2], sem_w.at[0]),
        pltpu.make_async_copy(wo_hbm, wo_all.at[y], sem_w.at[1]),
    ]
    for cp in loads:
        cp.start()

    y_up, y_dn, y_far = (y + 1) % 4, (y + 3) % 4, (y + 2) % 4
    peers = (at(z, x, c, y_up), at(z, x, c, y_dn))

    def greet(sem, devs):
        for dev in devs:
            pl.semaphore_signal(sem, inc=1, device_id=dev, device_id_type=MESH)
        pl.semaphore_wait(sem, len(devs))

    def along_z(n):
        return [at((z + n) % 16, x, c, y), at((z + 16 - n) % 16, x, c, y)]

    partner = at(z, x, 1 - c, y)
    sides = [at(z, (x + 1) % 4, c, y), at(z, (x + 3) % 4, c, y)]
    greet(pltpu.get_barrier_semaphore(), [*peers, partner, *sides, *along_z(1)])
    for cp in early:
        cp.wait()
    first = {}
    for h, d in ((0, 0), (1, 1), (1, 0), (0, 1)):
        cp = remote(tok_ref.at[h], tok_all.at[y, h], ysend, yrecv.at[d, h], peers[d])
        cp.start()
        first[d, h] = cp

    greet(hello.at[0], [*peers, partner, *along_z(1)])
    gain = gain_ref[...]

    def norm_rows(rows):
        rows = rows.astype(F32)
        inv = lax.rsqrt(jnp.mean(rows * rows, axis=1, keepdims=True) + RMS_EPS)
        return (rows * inv * gain).astype(BF16)

    for h in range(2):
        normed[y, pl.ds(h * 16, 16), :] = norm_rows(tok_ref[h])

    row_i = lax.broadcasted_iota(jnp.int32, (256, 256), 0)
    col_i = lax.broadcasted_iota(jnp.int32, (256, 256), 1)
    perm = jnp.where((row_i % 8) * 32 + row_i // 8 == col_i, 1.0, 0.0).astype(BF16)

    first[0, 0].wait_recv()
    relay0 = remote(tok_all.at[y_dn, 0], tok_all.at[y_dn, 0], ysend, y2recv.at[0], peers[0])
    relay0.start()
    first[1, 1].wait_recv()
    relay1 = remote(tok_all.at[y_up, 1], tok_all.at[y_up, 1], ysend, y2recv.at[1], peers[1])
    relay1.start()
    greet(hello.at[1], [partner, *along_z(2)])
    for dev in along_z(4):
        pl.semaphore_signal(hello.at[2], inc=1, device_id=dev, device_id_type=MESH)
    q_pad[...] = jnp.zeros((4, 256, 128), BF16)
    normed[y_dn, pl.ds(0, 16), :] = norm_rows(tok_all[y_dn, 0])
    normed[y_up, pl.ds(16, 16), :] = norm_rows(tok_all[y_up, 1])
    first[0, 1].wait_recv()
    normed[y_dn, pl.ds(16, 16), :] = norm_rows(tok_all[y_dn, 1])
    first[1, 0].wait_recv()
    normed[y_up, pl.ds(0, 16), :] = norm_rows(tok_all[y_up, 0])
    settle(w_qkv, sem_w.at[0])
    loads[3].wait()
    relay0.wait_recv()
    normed[y_far, pl.ds(0, 16), :] = norm_rows(tok_all[y_far, 0])
    relay1.wait_recv()
    normed[y_far, pl.ds(16, 16), :] = norm_rows(tok_all[y_far, 1])

    rows = normed[...].reshape(128, 2048)
    q = dot(rows, w_qkv[0])
    k = dot(rows, w_qkv[1])
    v = dot(rows, w_qkv[2])
    lane = lax.broadcasted_iota(jnp.int32, (128, 128), 1)
    low = lane < HEAD_DIM
    kv0 = jnp.where(low, k, pltpu.roll(v, HEAD_DIM, 1)).astype(BF16)
    kv1 = jnp.where(low, pltpu.roll(k, HEAD_DIM, 1), v).astype(BF16)
    mine0 = c == 0
    sib_out[0] = jnp.where(mine0, kv1, kv0)
    sib_out[1] = pltpu.roll(q, HEAD_DIM, 1).astype(BF16)
    sib = remote(sib_out, sib_in, bsend, brecv, at(z, x, 1 - c, y))
    sib.start()
    kv_mine = jnp.where(mine0, kv0, kv1)

    for yy in (y_up, y_dn, y_far):
        remote(wo_all.at[y, c], wo_all.at[y, c], wsend, wrecv, at(z, x, c, yy)).start()
    three_halves = wo_all.at[pl.ds(0, 3), 0]

    sib.wait_recv()
    q_first = (lane < HEAD_DIM) == mine0
    q_out[...] = jnp.where(q_first, q, sib_in[1].astype(F32)).astype(BF16)
    kv_sib = sib_in[0]
    pair = jnp.concatenate([jnp.where(mine0, kv_mine, kv_sib), jnp.where(mine0, kv_sib, kv_mine)], axis=0)
    kv_all[r, x] = dot(perm, pair).astype(BF16)

    def q_copy(n):
        return remote(q_out, q_in.at[n - 1], qsend, qrecv.at[n - 1], at((z + 16 - 4 * n) % 16, x, c, y))

    planes = (r, r + 1 - 2 * (r % 2), (r + 2) % 4, 3 - r)

    def z_copy(n):
        return remote(
            kv_all.at[r, x], kv_all.at[r, x], zsend, zrecv.at[n - 1], at(group * 4 + planes[n], x, c, y)
        )

    def x_copy(d, n):
        block = kv_all.at[planes[n], x]
        return remote(block, block, xsend, xrecv.at[d, n], sides[d])

    def x_relay(n):
        d = 0 if n < 2 else 1
        block = kv_all.at[planes[n], (x + (3 if d == 0 else 1)) % 4]
        return remote(block, block, xsend, x2recv.at[n], sides[d])

    def spread(n):
        if n:
            z_copy(n).wait_recv()
        x_copy(0, n).start()
        x_copy(1, n).start()

    def forward(n):
        x_copy(0 if n < 2 else 1, n).wait_recv()
        x_relay(n).start()

    low_half = lane < HEAD_DIM

    def complete(n):
        x_copy(1 if n < 2 else 0, n).wait_recv()
        x_relay(n).wait_recv()
        for b in range(4):
            vt_all[planes[n], :, pl.ds(b * 256, 256)] = (
                kv_all[planes[n], b].astype(F32).T[HEAD_DIM:, :].astype(BF16)
            )

    def pad_query(n, packed):
        packed = packed.astype(F32)
        q_pad[n, pl.ds(0, 128), :] = jnp.where(low_half, packed, 0.0).astype(BF16)
        q_pad[n, pl.ds(128, 128), :] = jnp.where(low_half, pltpu.roll(packed, HEAD_DIM, 1), 0.0).astype(BF16)

    def arrive(n):
        @pl.when(group + n <= 3)
        def _():
            q_copy(n).wait_recv()
            pad_query(n, q_in[n - 1])

    offset = off_ref[c] * LOG2E
    scale = HEAD_DIM ** (-0.5) * LOG2E
    sub = lax.broadcasted_iota(jnp.int32, (8, 512), 0)
    ahead = lax.broadcasted_iota(jnp.int32, (8, 256), 0) * 32 - lax.broadcasted_iota(jnp.int32, (8, 256), 1)

    def block(first_n, plane):
        sums = []
        for b in range(4):
            total = [None, None]
            for h in range(2):
                lanes = pl.ds(h * 256, 256)
                zz = lax.dot_general(kv_all[plane, b], q_pad[first_n + h], NT, preferred_element_type=F32)
                zz = zz.reshape(32, 8, 256)
                limit = x * 256 - b * 256 + (r - plane) * 1024
                for g in range(31, -1, -2):
                    up = []
                    for i in (g, g - 1):
                        e = jnp.exp2(jnp.minimum(zz[i] * scale + offset, 60.0))
                        if first_n + h == 0:
                            e = jnp.where(ahead < limit - i, e, 0.0)
                        e_s[b, i, :, lanes] = e
                        up.append(1.0 + e)
                    keep = jnp.log2(up[0] * up[1])
                    l_s[b, g // 2, :, lanes] = keep
                    total[h] = keep if total[h] is None else total[h] + keep
            sums.append(jnp.concatenate(total, axis=1))
        later = jnp.zeros((1, 512), F32)
        for b in range(3, -1, -1):
            total = sums[b]
            incl = total
            for step in (1, 2, 4):
                moved = pltpu.roll(incl, 8 - step, 0)
                incl = incl + jnp.where(sub < 8 - step, moved, 0.0)
            run = incl - total + later
            later = later + incl[0:1]
            for g in range(31, -1, -2):
                run = run + l_s[b, g // 2]
                left = jnp.exp2(-run)
                e = e_s[b, g - 1]
                w_s[b, g // 2] = jnp.concatenate([e * left, e_s[b, g] * (left * (1.0 + e))], axis=0).astype(BF16)
        o = dot(vt_all[plane], w_s[...].reshape(1024, 512))
        for h in range(2):
            part_o[first_n + h, plane] = o[:, h * 256 : h * 256 + 256]
            part_s[first_n + h, plane] = jnp.broadcast_to(later[:, h * 256 : h * 256 + 256], (8, 256))

    def near(n):
        @pl.when(jnp.logical_or(group < 3, planes[n] <= r))
        def _():
            block(0, planes[n])

        @pl.when(jnp.logical_and(group == 3, planes[n] > r))
        def _():
            part_o[0, planes[n]] = jnp.zeros((HEAD_DIM, 256), F32)
            part_s[0, planes[n]] = jnp.zeros((8, 256), F32)

    def far(n):
        @pl.when(group < 2)
        def _():
            block(2, planes[n])

    def finish(n):
        o = part_o[n, 3]
        s = part_s[n, 3][0:1]
        for plane in (2, 1, 0):
            o = o + jnp.exp2(-s) * part_o[n, plane]
            s = s + part_s[n, plane][0:1]
        return o, s

    def o_copy(n):
        dev = at((z + 4 * n) % 16, x, c, y)
        return (
            remote(o_out.at[n - 1], o_in.at[n - 1], osend, orecv.at[n - 1], dev),
            remote(s_out.at[n - 1], s_in.at[n - 1], ssend, srecv.at[n - 1], dev),
        )

    def give_back(n):
        @pl.when(group + n <= 3)
        def _():
            o, s = finish(n)
            o_out[n - 1] = o.astype(BF16)
            s_out[n - 1] = jnp.broadcast_to(s, (8, 256))
            for cp in o_copy(n):
                cp.start()

    def ask(n):
        @pl.when(group >= n)
        def _():
            q_copy(n).start()

    spread(0)
    z_copy(1).start()
    ask(1)
    z_copy(2).start()
    z_copy(3).start()
    ask(3)
    pad_query(0, q_out[...])
    forward(0)
    spread(1)
    pl.semaphore_wait(hello.at[2], 2)
    ask(2)
    spread(2)
    complete(0)
    forward(1)
    spread(3)
    arrive(1)
    near(0)
    forward(2)
    complete(1)
    near(1)
    forward(3)
    arrive(2)
    arrive(3)
    far(0)
    complete(2)
    far(1)
    near(2)
    complete(3)
    far(2)
    far(3)
    give_back(2)
    give_back(3)
    near(3)
    give_back(1)

    settle(three_halves, wrecv)
    for yy in (y_dn, y_up, y_far):
        remote(wo_all.at[yy, c], wo_all.at[yy, c], w2send, w2recv, partner).start()

    o, s = finish(0)
    acc_o[...] = o
    acc_s[...] = jnp.broadcast_to(s, (8, 256))
    for n in (1, 2, 3):
        @pl.when(group >= n)
        def _():
            for cp in o_copy(n):
                cp.wait_recv()
            s_ = acc_s[0:1, :]
            acc_o[...] += jnp.exp2(-s_) * o_in[n - 1].astype(F32)
            acc_s[...] += s_in[n - 1]

    o = acc_o[...]
    both = jnp.concatenate([jnp.where(mine0, o, 0.0), jnp.where(mine0, 0.0, o)], axis=0)
    att_out[...] = both.T.astype(BF16).reshape(8, 32, 128)
    for n in range(1, 8):
        cc = (c + n // 4) % 2
        yy = (y + n) % 4
        remote(att_out.at[cc * 4 + yy], att_in.at[y * 2 + c], asend, arecv, at(z, x, cc, yy)).start()
    att_in[y * 2 + c] = att_out[c * 4 + y]
    settle(three_halves, w2recv)
    settle(att_in.at[pl.ds(0, 7)], arecv)
    total = jnp.zeros((32, 2048), F32)
    for yy in range(4):
        feats = (att_in[2 * yy].astype(F32) + att_in[2 * yy + 1].astype(F32)).astype(BF16)
        part = dot(feats, wo_all[yy].reshape(128, 2048))
        total = total + part.astype(BF16).astype(F32)
    out_ref[...] = total.astype(BF16)

    settle(tok_all.at[pl.ds(0, 3)], ysend)
    sib.wait_send()
    settle(three_halves, wsend)
    settle(three_halves, w2send)
    settle(att_out.at[pl.ds(0, 7)], asend)
    settle(kv_all.at[0, pl.ds(0, 3)], zsend)
    settle(kv_all.at[pl.ds(0, 3)], xsend)
    for n in (1, 2, 3):
        @pl.when(group == n)
        def _():
            settle(q_in.at[pl.ds(0, n)], qsend)

        @pl.when(3 - group == n)
        def _():
            settle(o_in.at[pl.ds(0, n)], osend)
            settle(s_in.at[pl.ds(0, n)], ssend)


def per_device(tokens, norm_gain, w_query, w_key, w_value, score_offset, w_out):
    hbm = pl.BlockSpec(memory_space=pl.ANY)
    dma = pltpu.SemaphoreType.DMA
    v = pltpu.VMEM
    return pl.pallas_call(
        layer_kernel,
        out_shape=jax.ShapeDtypeStruct((32, 2048), BF16),
        in_specs=[hbm] * 7,
        out_specs=pl.BlockSpec(memory_space=pltpu.VMEM),
        scratch_shapes=[
            v((2, 16, 2048), BF16), v((1, 2048), F32), pltpu.SMEM((2,), F32),
            v((3, 2048, 128), BF16), v((4, 2, 64, 2048), BF16),
            v((4, 2, 16, 2048), BF16), v((4, 32, 2048), BF16),
            v((2, 128, 128), BF16), v((2, 128, 128), BF16),
            v((128, 128), BF16), v((3, 128, 128), BF16), v((4, 256, 128), BF16),
            v((4, 4, 256, 128), BF16), v((4, HEAD_DIM, 1024), BF16),
            v((4, 32, 8, 512), F32), v((4, 16, 8, 512), F32), v((4, 16, 16, 512), BF16),
            v((4, 4, HEAD_DIM, 256), F32), v((4, 4, 8, 256), F32),
            v((3, HEAD_DIM, 256), BF16), v((3, 8, 256), F32),
            v((3, HEAD_DIM, 256), BF16), v((3, 8, 256), F32),
            v((HEAD_DIM, 256), F32), v((8, 256), F32),
            v((8, 32, 128), BF16), v((8, 32, 128), BF16),
            dma((5,)), dma, dma((2, 2)), dma((2,)), dma, dma, dma, dma((3,)),
            dma, dma((3,)), dma, dma((2, 4)), dma((4,)),
            dma, dma((3,)), dma, dma((3,)),
            dma, dma, dma, dma, dma, dma, pltpu.SemaphoreType.REGULAR((3,)),
        ],
        compiler_params=pltpu.CompilerParams(has_side_effects=True, collective_id=0, vmem_limit_bytes=67043328),
    )(
        tokens.reshape(2, 16, 2048), norm_gain.reshape(1, 2048), score_offset,
        w_query, w_key, w_value, w_out.reshape(2, 64, 2048),
    )


def solution(mesh):
    rows = P(("sp", "tp"), None)
    placed = (rows, P(), P(None, "tp"), P(None, "tp"), P(None, "tp"), P("tp"), P("tp", None))
    return jax.shard_map(per_device, mesh=mesh, in_specs=placed, out_specs=rows, check_vma=False)
```

```python
import functools

import jax
import jax.numpy as jnp
from jax import lax
from jax.experimental import pallas as pl
from jax.experimental.pallas import tpu as pltpu
from jax.sharding import PartitionSpec as P

HEAD_DIM = 64
RMS_EPS = 1e-06
LOG2E = 1.4426950408889634
MESH = pl.DeviceIdType.MESH
NT = (((1,), (1,)), ((), ()))
NEG = -1e30
F32 = jnp.float32
BF16 = jnp.bfloat16


def dot(a, b):
    return jnp.dot(a, b, preferred_element_type=F32)


def layer_kernel(
    tok_hbm, gain_hbm, off_hbm, wq_hbm, wk_hbm, wv_hbm, wo_hbm, out_ref,
    tok_ref, gain_ref, off_ref, w_qkv, wo_all, tok_all, normed, sib_out, sib_in, q_out, q_in, q_pad,
    kv_all, vt_all, e_s, l_s, w_s, part_o, part_s, o_out, s_out, o_in, s_in, acc_o, acc_s,
    att_out, att_in,
    sem_w, ysend, yrecv, y2recv, bsend, brecv, qsend, qrecv,
    zsend, zrecv, xsend, xrecv, x2recv, osend, orecv, ssend, srecv,
    wsend, wrecv, w2send, w2recv, asend, arecv, hello,
):
    sp = lax.axis_index("sp")
    y = lax.axis_index("tp")
    z = sp // 8
    x = (sp // 2) % 4
    c = sp % 2
    group = z // 4
    r = z % 4

    def at(z_, x_, c_, y_):
        return ((z_ * 4 + x_) * 2 + c_, y_)

    def remote(src, dst, ss, rs, dev):
        return pltpu.make_async_remote_copy(
            src_ref=src, dst_ref=dst, send_sem=ss, recv_sem=rs, device_id=dev, device_id_type=MESH
        )

    def settle(ref, sem):
        pltpu.make_async_copy(ref, ref, sem).wait()

    early = [
        pltpu.make_async_copy(tok_hbm, tok_ref, sem_w.at[2]),
        pltpu.make_async_copy(gain_hbm, gain_ref, sem_w.at[3]),
        pltpu.make_async_copy(off_hbm, off_ref, sem_w.at[4]),
    ]
    for cp in early:
        cp.start()
    loads = [
        pltpu.make_async_copy(wq_hbm, w_qkv.at[0], sem_w.at[0]),
        pltpu.make_async_copy(wk_hbm, w_qkv.at[1], sem_w.at[0]),
        pltpu.make_async_copy(wv_hbm, w_qkv.at[2], sem_w.at[0]),
        pltpu.make_async_copy(wo_hbm, wo_all.at[y], sem_w.at[1]),
    ]
    for cp in loads:
        cp.start()

    y_up, y_dn, y_far = (y + 1) % 4, (y + 3) % 4, (y + 2) % 4
    peers = (at(z, x, c, y_up), at(z, x, c, y_dn))

    def greet(sem, devs):
        for dev in devs:
            pl.semaphore_signal(sem, inc=1, device_id=dev, device_id_type=MESH)
        pl.semaphore_wait(sem, len(devs))

    def along_z(n):
        return [at((z + n) % 16, x, c, y), at((z + 16 - n) % 16, x, c, y)]

    partner = at(z, x, 1 - c, y)
    sides = [at(z, (x + 1) % 4, c, y), at(z, (x + 3) % 4, c, y)]
    greet(pltpu.get_barrier_semaphore(), [*peers, partner, *sides, *along_z(1)])
    for cp in early:
        cp.wait()
    first = {}
    for h, d in ((0, 0), (1, 1), (1, 0), (0, 1)):
        cp = remote(tok_ref.at[h], tok_all.at[y, h], ysend, yrecv.at[d, h], peers[d])
        cp.start()
        first[d, h] = cp

    greet(hello.at[0], [*peers, partner, *along_z(1)])
    gain = gain_ref[...]

    def norm_rows(rows):
        rows = rows.astype(F32)
        inv = lax.rsqrt(jnp.mean(rows * rows, axis=1, keepdims=True) + RMS_EPS)
        return (rows * inv * gain).astype(BF16)

    for h in range(2):
        normed[y, pl.ds(h * 16, 16), :] = norm_rows(tok_ref[h])

    row_i = lax.broadcasted_iota(jnp.int32, (256, 256), 0)
    col_i = lax.broadcasted_iota(jnp.int32, (256, 256), 1)
    perm = jnp.where((row_i % 8) * 32 + row_i // 8 == col_i, 1.0, 0.0).astype(BF16)

    first[0, 0].wait_recv()
    relay0 = remote(tok_all.at[y_dn, 0], tok_all.at[y_dn, 0], ysend, y2recv.at[0], peers[0])
    relay0.start()
    first[1, 1].wait_recv()
    relay1 = remote(tok_all.at[y_up, 1], tok_all.at[y_up, 1], ysend, y2recv.at[1], peers[1])
    relay1.start()
    greet(hello.at[1], [partner, *along_z(2)])
    for dev in along_z(4):
        pl.semaphore_signal(hello.at[2], inc=1, device_id=dev, device_id_type=MESH)
    q_pad[...] = jnp.zeros((4, 256, 128), BF16)
    normed[y_dn, pl.ds(0, 16), :] = norm_rows(tok_all[y_dn, 0])
    normed[y_up, pl.ds(16, 16), :] = norm_rows(tok_all[y_up, 1])
    first[0, 1].wait_recv()
    normed[y_dn, pl.ds(16, 16), :] = norm_rows(tok_all[y_dn, 1])
    first[1, 0].wait_recv()
    normed[y_up, pl.ds(0, 16), :] = norm_rows(tok_all[y_up, 0])
    settle(w_qkv, sem_w.at[0])
    loads[3].wait()
    relay0.wait_recv()
    normed[y_far, pl.ds(0, 16), :] = norm_rows(tok_all[y_far, 0])
    relay1.wait_recv()
    normed[y_far, pl.ds(16, 16), :] = norm_rows(tok_all[y_far, 1])

    rows = normed[...].reshape(128, 2048)
    q = dot(rows, w_qkv[0])
    k = dot(rows, w_qkv[1])
    v = dot(rows, w_qkv[2])
    lane = lax.broadcasted_iota(jnp.int32, (128, 128), 1)
    low = lane < HEAD_DIM
    kv0 = jnp.where(low, k, pltpu.roll(v, HEAD_DIM, 1)).astype(BF16)
    kv1 = jnp.where(low, pltpu.roll(k, HEAD_DIM, 1), v).astype(BF16)
    mine0 = c == 0
    sib_out[0] = jnp.where(mine0, kv1, kv0)
    sib_out[1] = pltpu.roll(q, HEAD_DIM, 1).astype(BF16)
    sib = remote(sib_out, sib_in, bsend, brecv, at(z, x, 1 - c, y))
    sib.start()
    kv_mine = jnp.where(mine0, kv0, kv1)

    for yy in (y_up, y_dn, y_far):
        remote(wo_all.at[y, c], wo_all.at[y, c], wsend, wrecv, at(z, x, c, yy)).start()
    three_halves = wo_all.at[pl.ds(0, 3), 0]

    sib.wait_recv()
    q_first = (lane < HEAD_DIM) == mine0
    q_out[...] = jnp.where(q_first, q, sib_in[1].astype(F32)).astype(BF16)
    kv_sib = sib_in[0]
    pair = jnp.concatenate([jnp.where(mine0, kv_mine, kv_sib), jnp.where(mine0, kv_sib, kv_mine)], axis=0)
    kv_all[r, x] = dot(perm, pair).astype(BF16)

    def q_copy(n):
        return remote(q_out, q_in.at[n - 1], qsend, qrecv.at[n - 1], at((z + 16 - 4 * n) % 16, x, c, y))

    planes = (r, r + 1 - 2 * (r % 2), (r + 2) % 4, 3 - r)

    def z_copy(n):
        return remote(
            kv_all.at[r, x], kv_all.at[r, x], zsend, zrecv.at[n - 1], at(group * 4 + planes[n], x, c, y)
        )

    def x_copy(d, n):
        block = kv_all.at[planes[n], x]
        return remote(block, block, xsend, xrecv.at[d, n], sides[d])

    def x_relay(n):
        d = 0 if n < 2 else 1
        block = kv_all.at[planes[n], (x + (3 if d == 0 else 1)) % 4]
        return remote(block, block, xsend, x2recv.at[n], sides[d])

    def spread(n):
        if n:
            z_copy(n).wait_recv()
        x_copy(0, n).start()
        x_copy(1, n).start()

    def forward(n):
        x_copy(0 if n < 2 else 1, n).wait_recv()
        x_relay(n).start()

    low_half = lane < HEAD_DIM

    def complete(n):
        x_copy(1 if n < 2 else 0, n).wait_recv()
        x_relay(n).wait_recv()
        for b in range(4):
            vt_all[planes[n], :, pl.ds(b * 256, 256)] = (
                kv_all[planes[n], b].astype(F32).T[HEAD_DIM:, :].astype(BF16)
            )

    def pad_query(n, packed):
        packed = packed.astype(F32)
        q_pad[n, pl.ds(0, 128), :] = jnp.where(low_half, packed, 0.0).astype(BF16)
        q_pad[n, pl.ds(128, 128), :] = jnp.where(low_half, pltpu.roll(packed, HEAD_DIM, 1), 0.0).astype(BF16)

    def arrive(n):
        @pl.when(group + n <= 3)
        def _():
            q_copy(n).wait_recv()
            pad_query(n, q_in[n - 1])

    offset = off_ref[c] * LOG2E
    scale = HEAD_DIM ** (-0.5) * LOG2E
    ahead = lax.broadcasted_iota(jnp.int32, (8, 256), 0) * 32 - lax.broadcasted_iota(jnp.int32, (8, 256), 1)

    def block(*pairs):
        pairs = [(n, planes[m]) for n, m in pairs]
        wide = 256 * len(pairs)
        every = pl.ds(0, wide)
        sub = lax.broadcasted_iota(jnp.int32, (8, wide), 0)
        sums = []
        for b in range(4):
            total = [None] * len(pairs)
            for h, (n, plane) in enumerate(pairs):
                lanes = pl.ds(h * 256, 256)
                zz = lax.dot_general(kv_all[plane, b], q_pad[n], NT, preferred_element_type=F32)
                zz = zz.reshape(32, 8, 256)
                limit = x * 256 - b * 256 + (r - plane) * 1024
                for g in range(31, -1, -2):
                    up = []
                    for i in (g, g - 1):
                        e = jnp.exp2(jnp.minimum(zz[i] * scale + offset, 60.0))
                        if n == 0:
                            e = jnp.where(ahead < limit - i, e, 0.0)
                        e_s[b, i, :, lanes] = e
                        up.append(1.0 + e)
                    keep = jnp.log2(up[0] * up[1])
                    l_s[b, g // 2, :, lanes] = keep
                    total[h] = keep if total[h] is None else total[h] + keep
            sums.append(jnp.concatenate(total, axis=1))
        later = jnp.zeros((1, wide), F32)
        for b in range(3, -1, -1):
            total = sums[b]
            incl = total
            for step in (1, 2, 4):
                moved = pltpu.roll(incl, 8 - step, 0)
                incl = incl + jnp.where(sub < 8 - step, moved, 0.0)
            run = incl - total + later
            later = later + incl[0:1]
            for g in range(31, -1, -2):
                run = run + l_s[b, g // 2, :, every]
                left = jnp.exp2(-run)
                e = e_s[b, g - 1, :, every]
                w_s[b, g // 2, :, every] = jnp.concatenate(
                    [e * left, e_s[b, g, :, every] * (left * (1.0 + e))], axis=0
                ).astype(BF16)
        for h, (n, plane) in enumerate(pairs):
            part_o[n, plane] = dot(vt_all[plane], w_s[:, :, :, pl.ds(h * 256, 256)].reshape(1024, 256))
            part_s[n, plane] = jnp.broadcast_to(later[:, h * 256 : h * 256 + 256], (8, 256))

    def own(n):
        @pl.when(planes[n] <= r)
        def _():
            block((0, n))

        @pl.when(planes[n] > r)
        def _():
            part_o[0, planes[n]] = jnp.zeros((HEAD_DIM, 256), F32)
            part_s[0, planes[n]] = jnp.zeros((8, 256), F32)

    def near_groups(first, *pairs):
        @pl.when(jnp.logical_and(group >= first, group < 3))
        def _():
            block(*pairs)

    def group_is(g, *pairs):
        @pl.when(group == g)
        def _():
            block(*pairs)

    def two_groups(*pairs):
        @pl.when(group < 2)
        def _():
            block(*pairs)

    def finish(n):
        o = part_o[n, 3]
        s = part_s[n, 3][0:1]
        for plane in (2, 1, 0):
            o = o + jnp.exp2(-s) * part_o[n, plane]
            s = s + part_s[n, plane][0:1]
        return o, s

    def o_copy(n):
        dev = at((z + 4 * n) % 16, x, c, y)
        return (
            remote(o_out.at[n - 1], o_in.at[n - 1], osend, orecv.at[n - 1], dev),
            remote(s_out.at[n - 1], s_in.at[n - 1], ssend, srecv.at[n - 1], dev),
        )

    def give_back(n):
        @pl.when(group + n <= 3)
        def _():
            o, s = finish(n)
            o_out[n - 1] = o.astype(BF16)
            s_out[n - 1] = s
            for cp in o_copy(n):
                cp.start()

    def ask(n):
        @pl.when(group >= n)
        def _():
            q_copy(n).start()

    spread(0)
    z_copy(1).start()
    ask(1)
    z_copy(2).start()
    z_copy(3).start()
    ask(3)
    pad_query(0, q_out[...])
    forward(0)
    spread(1)
    pl.semaphore_wait(hello.at[2], 2)
    ask(2)
    spread(2)
    complete(0)
    spread(3)
    forward(1)
    own(0)
    forward(2)
    arrive(1)
    arrive(3)
    group_is(0, (1, 0), (3, 0))
    forward(3)
    complete(1)
    group_is(0, (1, 1), (3, 1))
    near_groups(1, (1, 0), (1, 1))
    arrive(2)
    complete(2)
    two_groups((2, 0), (2, 1), (2, 2))
    complete(3)
    group_is(0, (2, 3), (1, 2), (3, 2))
    group_is(1, (2, 3), (1, 2))
    give_back(2)
    group_is(0, (1, 3), (3, 3))
    give_back(3)
    group_is(1, (1, 3))
    group_is(2, (1, 2), (1, 3))
    give_back(1)
    own(1)
    own(2)
    own(3)

    settle(three_halves, wrecv)
    for yy in (y_dn, y_up, y_far):
        remote(wo_all.at[yy, c], wo_all.at[yy, c], w2send, w2recv, partner).start()

    o, s = finish(0)
    acc_o[...] = o
    acc_s[...] = jnp.broadcast_to(s, (8, 256))
    for n in (1, 2, 3):
        @pl.when(group >= n)
        def _():
            for cp in o_copy(n):
                cp.wait_recv()
            s_ = acc_s[0:1, :]
            acc_o[...] += jnp.exp2(-s_) * o_in[n - 1].astype(F32)
            acc_s[...] = jnp.broadcast_to(s_ + s_in[n - 1], (8, 256))

    o = acc_o[...]
    both = jnp.concatenate([jnp.where(mine0, o, 0.0), jnp.where(mine0, 0.0, o)], axis=0)
    att_out[...] = both.T.astype(BF16).reshape(8, 32, 128)
    for n in range(1, 8):
        cc = (c + n // 4) % 2
        yy = (y + n) % 4
        remote(att_out.at[cc * 4 + yy], att_in.at[y * 2 + c], asend, arecv, at(z, x, cc, yy)).start()
    att_in[y * 2 + c] = att_out[c * 4 + y]
    settle(three_halves, w2recv)
    settle(att_in.at[pl.ds(0, 7)], arecv)
    total = jnp.zeros((32, 2048), F32)
    for yy in range(4):
        feats = (att_in[2 * yy].astype(F32) + att_in[2 * yy + 1].astype(F32)).astype(BF16)
        part = dot(feats, wo_all[yy].reshape(128, 2048))
        total = total + part.astype(BF16).astype(F32)
    out_ref[...] = total.astype(BF16)

    settle(tok_all.at[pl.ds(0, 3)], ysend)
    sib.wait_send()
    settle(three_halves, wsend)
    settle(three_halves, w2send)
    settle(att_out.at[pl.ds(0, 7)], asend)
    settle(kv_all.at[0, pl.ds(0, 3)], zsend)
    settle(kv_all.at[pl.ds(0, 3)], xsend)
    for n in (1, 2, 3):
        @pl.when(group == n)
        def _():
            settle(q_in.at[pl.ds(0, n)], qsend)

        @pl.when(3 - group == n)
        def _():
            settle(o_in.at[pl.ds(0, n)], osend)
            settle(s_in.at[pl.ds(0, n)], ssend)


def per_device(tokens, norm_gain, w_query, w_key, w_value, score_offset, w_out):
    hbm = pl.BlockSpec(memory_space=pl.ANY)
    dma = pltpu.SemaphoreType.DMA
    v = pltpu.VMEM
    return pl.pallas_call(
        layer_kernel,
        out_shape=jax.ShapeDtypeStruct((32, 2048), BF16),
        in_specs=[hbm] * 7,
        out_specs=pl.BlockSpec(memory_space=pltpu.VMEM),
        scratch_shapes=[
            v((2, 16, 2048), BF16), v((1, 2048), F32), pltpu.SMEM((2,), F32),
            v((3, 2048, 128), BF16), v((4, 2, 64, 2048), BF16),
            v((4, 2, 16, 2048), BF16), v((4, 32, 2048), BF16),
            v((2, 128, 128), BF16), v((2, 128, 128), BF16),
            v((128, 128), BF16), v((3, 128, 128), BF16), v((4, 256, 128), BF16),
            v((4, 4, 256, 128), BF16), v((4, HEAD_DIM, 1024), BF16),
            v((4, 32, 8, 768), F32), v((4, 16, 8, 768), F32), v((4, 16, 16, 768), BF16),
            v((4, 4, HEAD_DIM, 256), F32), v((4, 4, 8, 256), F32),
            v((3, HEAD_DIM, 256), BF16), v((3, 1, 256), F32),
            v((3, HEAD_DIM, 256), BF16), v((3, 1, 256), F32),
            v((HEAD_DIM, 256), F32), v((8, 256), F32),
            v((8, 32, 128), BF16), v((8, 32, 128), BF16),
            dma((5,)), dma, dma((2, 2)), dma((2,)), dma, dma, dma, dma((3,)),
            dma, dma((3,)), dma, dma((2, 4)), dma((4,)),
            dma, dma((3,)), dma, dma((3,)),
            dma, dma, dma, dma, dma, dma, pltpu.SemaphoreType.REGULAR((3,)),
        ],
        compiler_params=pltpu.CompilerParams(has_side_effects=True, collective_id=0, vmem_limit_bytes=67043328),
    )(
        tokens.reshape(2, 16, 2048), norm_gain.reshape(1, 2048), score_offset,
        w_query, w_key, w_value, w_out.reshape(2, 64, 2048),
    )


def solution(mesh):
    rows = P(("sp", "tp"), None)
    placed = (rows, P(), P(None, "tp"), P(None, "tp"), P(None, "tp"), P("tp"), P("tp", None))
    return jax.shard_map(per_device, mesh=mesh, in_specs=placed, out_specs=rows, check_vma=False)
```

```python
import functools

import jax
import jax.numpy as jnp
from jax import lax
from jax.experimental import pallas as pl
from jax.experimental.pallas import tpu as pltpu
from jax.sharding import PartitionSpec as P

HEAD_DIM = 64
RMS_EPS = 1e-06
LOG2E = 1.4426950408889634
MESH = pl.DeviceIdType.MESH
NT = (((1,), (1,)), ((), ()))
NEG = -1e30
F32 = jnp.float32
BF16 = jnp.bfloat16


def dot(a, b):
    return jnp.dot(a, b, preferred_element_type=F32)


def layer_kernel(
    tok_hbm, gain_hbm, off_hbm, wq_hbm, wk_hbm, wv_hbm, wo_hbm, out_ref,
    tok_ref, gain_ref, off_ref, w_qkv, wo_all, tok_all, normed, sib_out, sib_in, q_out, q_in, q_pad,
    kv_all, vt_all, e_s, l_s, w_s, part_o, part_s, o_out, s_out, o_in, s_in, acc_o, acc_s,
    att_out, att_in,
    sem_w, ysend, yrecv, y2recv, bsend, brecv, qsend, qrecv,
    zsend, zrecv, xsend, xrecv, x2recv, osend, orecv, ssend, srecv,
    wsend, wrecv, w2send, w2recv, asend, arecv, hello,
):
    sp = lax.axis_index("sp")
    y = lax.axis_index("tp")
    z = sp // 8
    x = (sp // 2) % 4
    c = sp % 2
    group = z // 4
    r = z % 4

    def at(z_, x_, c_, y_):
        return ((z_ * 4 + x_) * 2 + c_, y_)

    def remote(src, dst, ss, rs, dev):
        return pltpu.make_async_remote_copy(
            src_ref=src, dst_ref=dst, send_sem=ss, recv_sem=rs, device_id=dev, device_id_type=MESH
        )

    def settle(ref, sem):
        pltpu.make_async_copy(ref, ref, sem).wait()

    early = [
        pltpu.make_async_copy(tok_hbm, tok_ref, sem_w.at[2]),
        pltpu.make_async_copy(gain_hbm, gain_ref, sem_w.at[3]),
        pltpu.make_async_copy(off_hbm, off_ref, sem_w.at[4]),
    ]
    for cp in early:
        cp.start()
    loads = [
        pltpu.make_async_copy(wq_hbm, w_qkv.at[0], sem_w.at[0]),
        pltpu.make_async_copy(wk_hbm, w_qkv.at[1], sem_w.at[0]),
        pltpu.make_async_copy(wv_hbm, w_qkv.at[2], sem_w.at[0]),
        pltpu.make_async_copy(wo_hbm, wo_all.at[y], sem_w.at[1]),
    ]
    for cp in loads:
        cp.start()

    y_up, y_dn, y_far = (y + 1) % 4, (y + 3) % 4, (y + 2) % 4
    peers = (at(z, x, c, y_up), at(z, x, c, y_dn))

    def greet(sem, devs):
        for dev in devs:
            pl.semaphore_signal(sem, inc=1, device_id=dev, device_id_type=MESH)
        pl.semaphore_wait(sem, len(devs))

    def along_z(n):
        return [at((z + n) % 16, x, c, y), at((z + 16 - n) % 16, x, c, y)]

    partner = at(z, x, 1 - c, y)
    sides = [at(z, (x + 1) % 4, c, y), at(z, (x + 3) % 4, c, y)]
    greet(pltpu.get_barrier_semaphore(), [*peers, partner, *sides, *along_z(1)])
    for cp in early:
        cp.wait()
    cols = (pl.ds(0, 1024), pl.ds(1024, 1024))
    first = {}
    for n in range(2):
        for d in range(2):
            first[d, n] = remote(
                tok_ref.at[d, :, cols[n]], tok_all.at[y, d, :, cols[n]], ysend, yrecv.at[d, n], peers[d]
            )
    for d in range(2):
        first[d, 2] = remote(tok_ref.at[1 - d], tok_all.at[y, 1 - d], ysend, yrecv.at[d, 2], peers[d])
    for cp in first.values():
        cp.start()

    greet(hello.at[0], [*peers, partner, *sides, *along_z(1)])
    gain = gain_ref[...]

    def norm_rows(rows):
        rows = rows.astype(F32)
        inv = lax.rsqrt(jnp.mean(rows * rows, axis=1, keepdims=True) + RMS_EPS)
        return (rows * inv * gain).astype(BF16)

    for h in range(2):
        normed[y, pl.ds(h * 16, 16), :] = norm_rows(tok_ref[h])

    row_i = lax.broadcasted_iota(jnp.int32, (256, 256), 0)
    col_i = lax.broadcasted_iota(jnp.int32, (256, 256), 1)
    perm = jnp.where((row_i % 8) * 32 + row_i // 8 == col_i, 1.0, 0.0).astype(BF16)

    relays = []
    for n in range(2):
        for d in range(2):
            first[d, n].wait_recv()
            piece = tok_all.at[(y_dn, y_up)[d], d, :, cols[n]]
            relays.append(remote(piece, piece, ysend, y2recv.at[d, n], peers[d]))
            relays[-1].start()
    greet(hello.at[1], [partner, *along_z(2)])
    for dev in along_z(4):
        pl.semaphore_signal(hello.at[2], inc=1, device_id=dev, device_id_type=MESH)
    q_pad[...] = jnp.zeros((4, 256, 128), BF16)
    normed[y_dn, pl.ds(0, 16), :] = norm_rows(tok_all[y_dn, 0])
    normed[y_up, pl.ds(16, 16), :] = norm_rows(tok_all[y_up, 1])
    first[0, 2].wait_recv()
    normed[y_dn, pl.ds(16, 16), :] = norm_rows(tok_all[y_dn, 1])
    first[1, 2].wait_recv()
    normed[y_up, pl.ds(0, 16), :] = norm_rows(tok_all[y_up, 0])
    settle(w_qkv, sem_w.at[0])
    loads[3].wait()
    for d in range(2):
        relays[d].wait_recv()
        relays[d + 2].wait_recv()
        normed[y_far, pl.ds(16 * d, 16), :] = norm_rows(tok_all[y_far, d])

    rows = normed[...].reshape(128, 2048)
    q = dot(rows, w_qkv[0])
    k = dot(rows, w_qkv[1])
    v = dot(rows, w_qkv[2])
    lane = lax.broadcasted_iota(jnp.int32, (128, 128), 1)
    low = lane < HEAD_DIM
    kv0 = jnp.where(low, k, pltpu.roll(v, HEAD_DIM, 1)).astype(BF16)
    kv1 = jnp.where(low, pltpu.roll(k, HEAD_DIM, 1), v).astype(BF16)
    mine0 = c == 0
    sib_out[0] = jnp.where(mine0, kv1, kv0)
    sib_out[1] = pltpu.roll(q, HEAD_DIM, 1).astype(BF16)
    sib = remote(sib_out, sib_in, bsend, brecv, at(z, x, 1 - c, y))
    sib.start()
    kv_mine = jnp.where(mine0, kv0, kv1)

    for yy in (y_up, y_dn, y_far):
        remote(wo_all.at[y, c], wo_all.at[y, c], wsend, wrecv, at(z, x, c, yy)).start()
    three_halves = wo_all.at[pl.ds(0, 3), 0]

    sib.wait_recv()
    q_first = (lane < HEAD_DIM) == mine0
    q_out[...] = jnp.where(q_first, q, sib_in[1].astype(F32)).astype(BF16)
    kv_sib = sib_in[0]
    pair = jnp.concatenate([jnp.where(mine0, kv_mine, kv_sib), jnp.where(mine0, kv_sib, kv_mine)], axis=0)
    kv_all[r, x] = dot(perm, pair).astype(BF16)

    below = {1: (z + 12) % 16, 2: (z + 27 - 2 * r) % 16, 3: (z + 4) % 16}
    above = {1: (z + 4) % 16, 2: (z + 27 - 2 * r) % 16, 3: (z + 12) % 16}

    def q_copy(n):
        return remote(q_out, q_in.at[n - 1], qsend, qrecv.at[n - 1], at(below[n], x, c, y))

    planes = (r, r + 1 - 2 * (r % 2), (r + 2) % 4, 3 - r)

    def z_copy(n):
        return remote(
            kv_all.at[r, x], kv_all.at[r, x], zsend, zrecv.at[n - 1], at(group * 4 + planes[n], x, c, y)
        )

    def x_copy(d, n):
        block = kv_all.at[planes[n], x]
        return remote(block, block, xsend, xrecv.at[d, n], sides[d])

    def x_relay(n):
        if n < 2:
            block = kv_all.at[planes[n], (x + (3, 1)[n]) % 4]
            return remote(block, block, xsend, x2recv.at[n], sides[n])
        block = kv_all.at[planes[n], x]
        return remote(block, block, xsend, x2recv.at[n], at(z, (x + 2) % 4, c, y))

    def spread(n):
        if n:
            z_copy(n).wait_recv()
        x_copy(0, n).start()
        x_copy(1, n).start()
        if n >= 2:
            x_relay(n).start()

    def forward(n):
        x_copy(n, n).wait_recv()
        x_relay(n).start()

    low_half = lane < HEAD_DIM

    def complete(n):
        for d in range(2):
            if d != n:
                x_copy(d, n).wait_recv()
        x_relay(n).wait_recv()
        for b in range(4):
            vt_all[planes[n], :, pl.ds(b * 256, 256)] = (
                kv_all[planes[n], b].astype(F32).T[HEAD_DIM:, :].astype(BF16)
            )

    def pad_query(n, packed):
        packed = packed.astype(F32)
        q_pad[n, pl.ds(0, 128), :] = jnp.where(low_half, packed, 0.0).astype(BF16)
        q_pad[n, pl.ds(128, 128), :] = jnp.where(low_half, pltpu.roll(packed, HEAD_DIM, 1), 0.0).astype(BF16)

    def arrive(n):
        @pl.when(group + n <= 3)
        def _():
            q_copy(n).wait_recv()
            pad_query(n, q_in[n - 1])

    offset = off_ref[c] * LOG2E
    scale = HEAD_DIM ** (-0.5) * LOG2E
    ahead = lax.broadcasted_iota(jnp.int32, (8, 256), 0) * 32 - lax.broadcasted_iota(jnp.int32, (8, 256), 1)

    def block(*pairs):
        pairs = [(n, planes[m]) for n, m in pairs]
        wide = 256 * len(pairs)
        every = pl.ds(0, wide)
        sub = lax.broadcasted_iota(jnp.int32, (8, wide), 0)
        sums = []
        for b in range(4):
            total = [None] * len(pairs)
            for h, (n, plane) in enumerate(pairs):
                lanes = pl.ds(h * 256, 256)
                zz = lax.dot_general(kv_all[plane, b], q_pad[n], NT, preferred_element_type=F32)
                zz = zz.reshape(32, 8, 256)
                limit = x * 256 - b * 256 + (r - plane) * 1024
                for g in range(31, -1, -2):
                    up = []
                    for i in (g, g - 1):
                        e = jnp.exp2(jnp.minimum(zz[i] * scale + offset, 60.0))
                        if n == 0:
                            e = jnp.where(ahead < limit - i, e, 0.0)
                        e_s[b, i, :, lanes] = e
                        up.append(1.0 + e)
                    keep = jnp.log2(up[0] * up[1])
                    l_s[b, g // 2, :, lanes] = keep
                    total[h] = keep if total[h] is None else total[h] + keep
            sums.append(jnp.concatenate(total, axis=1))
        later = jnp.zeros((1, wide), F32)
        for b in range(3, -1, -1):
            total = sums[b]
            incl = total
            for step in (1, 2, 4):
                moved = pltpu.roll(incl, 8 - step, 0)
                incl = incl + jnp.where(sub < 8 - step, moved, 0.0)
            run = incl - total + later
            later = later + incl[0:1]
            for g in range(31, -1, -2):
                run = run + l_s[b, g // 2, :, every]
                left = jnp.exp2(-run)
                e = e_s[b, g - 1, :, every]
                w_s[b, g // 2, :, every] = jnp.concatenate(
                    [e * left, e_s[b, g, :, every] * (left * (1.0 + e))], axis=0
                ).astype(BF16)
        for h, (n, plane) in enumerate(pairs):
            part_o[n, plane] = dot(vt_all[plane], w_s[:, :, :, pl.ds(h * 256, 256)].reshape(1024, 256))
            part_s[n, plane] = jnp.broadcast_to(later[:, h * 256 : h * 256 + 256], (8, 256))

    for m in (1, 2, 3):
        @pl.when(planes[m] > r)
        def _():
            part_o[0, planes[m]] = jnp.zeros((HEAD_DIM, 256), F32)
            part_s[0, planes[m]] = jnp.zeros((8, 256), F32)

    def own_rest():
        for plane, pairs in ((1, ((0, 1),)), (2, ((0, 2), (0, 3))), (3, ((0, 1), (0, 2), (0, 3)))):
            @pl.when(r == plane)
            def _():
                block(*pairs)

    def near_groups(first, *pairs):
        @pl.when(jnp.logical_and(group >= first, group < 3))
        def _():
            block(*pairs)

    def group_is(g, *pairs):
        @pl.when(group == g)
        def _():
            block(*pairs)

    def two_groups(*pairs):
        @pl.when(group < 2)
        def _():
            block(*pairs)

    def finish(n):
        o = part_o[n, 3]
        s = part_s[n, 3][0:1]
        for plane in (2, 1, 0):
            o = o + jnp.exp2(-s) * part_o[n, plane]
            s = s + part_s[n, plane][0:1]
        return o, s

    def o_copy(n):
        dev = at(above[n], x, c, y)
        return (
            remote(o_out.at[n - 1], o_in.at[n - 1], osend, orecv.at[n - 1], dev),
            remote(s_out.at[n - 1], s_in.at[n - 1], ssend, srecv.at[n - 1], dev),
        )

    def give_back(n):
        @pl.when(group + n <= 3)
        def _():
            o, s = finish(n)
            o_out[n - 1] = o.astype(BF16)
            s_out[n - 1] = s
            for cp in o_copy(n):
                cp.start()

    def ask(n):
        @pl.when(group >= n)
        def _():
            q_copy(n).start()

    spread(0)
    z_copy(1).start()
    z_copy(2).start()
    z_copy(3).start()
    pl.semaphore_wait(hello.at[2], 2)
    ask(2)
    ask(1)
    ask(3)
    pad_query(0, q_out[...])
    forward(0)
    spread(1)
    spread(2)
    complete(0)
    forward(1)
    block((0, 0))
    spread(3)
    arrive(2)
    two_groups((2, 0))
    arrive(1)
    arrive(3)
    group_is(0, (1, 0), (3, 0))
    group_is(1, (1, 0))
    complete(1)
    group_is(0, (2, 1), (1, 1), (3, 1))
    group_is(1, (2, 1), (1, 1))
    group_is(2, (1, 0), (1, 1))
    complete(2)
    group_is(0, (2, 2), (1, 2), (3, 2))
    group_is(1, (2, 2), (1, 2))
    complete(3)
    two_groups((2, 3))
    give_back(2)
    group_is(0, (1, 3), (3, 3))
    give_back(3)
    group_is(1, (1, 3))
    group_is(2, (1, 2), (1, 3))
    give_back(1)
    own_rest()

    settle(three_halves, wrecv)
    for yy in (y_dn, y_up, y_far):
        remote(wo_all.at[yy, c], wo_all.at[yy, c], w2send, w2recv, partner).start()

    o, s = finish(0)
    acc_o[...] = o
    acc_s[...] = jnp.broadcast_to(s, (8, 256))
    for n in (1, 2, 3):
        @pl.when(group >= n)
        def _():
            for cp in o_copy(n):
                cp.wait_recv()
            s_ = acc_s[0:1, :]
            acc_o[...] += jnp.exp2(-s_) * o_in[n - 1].astype(F32)
            acc_s[...] = jnp.broadcast_to(s_ + s_in[n - 1], (8, 256))

    o = acc_o[...]
    both = jnp.concatenate([jnp.where(mine0, o, 0.0), jnp.where(mine0, 0.0, o)], axis=0)
    att_out[...] = both.T.astype(BF16).reshape(8, 32, 128)
    for n in range(1, 8):
        cc = (c + n // 4) % 2
        yy = (y + n) % 4
        remote(att_out.at[cc * 4 + yy], att_in.at[y * 2 + c], asend, arecv, at(z, x, cc, yy)).start()
    att_in[y * 2 + c] = att_out[c * 4 + y]
    settle(three_halves, w2recv)
    settle(att_in.at[pl.ds(0, 7)], arecv)
    total = jnp.zeros((32, 2048), F32)
    for yy in range(4):
        feats = (att_in[2 * yy].astype(F32) + att_in[2 * yy + 1].astype(F32)).astype(BF16)
        part = dot(feats, wo_all[yy].reshape(128, 2048))
        total = total + part.astype(BF16).astype(F32)
    out_ref[...] = total.astype(BF16)

    settle(tok_all.at[pl.ds(0, 3)], ysend)
    sib.wait_send()
    settle(three_halves, wsend)
    settle(three_halves, w2send)
    settle(att_out.at[pl.ds(0, 7)], asend)
    settle(kv_all.at[0, pl.ds(0, 3)], zsend)
    settle(kv_all.at[pl.ds(0, 3)], xsend)
    for n in (1, 2, 3):
        @pl.when(group == n)
        def _():
            settle(q_in.at[pl.ds(0, n)], qsend)

        @pl.when(3 - group == n)
        def _():
            settle(o_in.at[pl.ds(0, n)], osend)
            settle(s_in.at[pl.ds(0, n)], ssend)


def per_device(tokens, norm_gain, w_query, w_key, w_value, score_offset, w_out):
    hbm = pl.BlockSpec(memory_space=pl.ANY)
    dma = pltpu.SemaphoreType.DMA
    v = pltpu.VMEM
    return pl.pallas_call(
        layer_kernel,
        out_shape=jax.ShapeDtypeStruct((32, 2048), BF16),
        in_specs=[hbm] * 7,
        out_specs=pl.BlockSpec(memory_space=pltpu.VMEM),
        scratch_shapes=[
            v((2, 16, 2048), BF16), v((1, 2048), F32), pltpu.SMEM((2,), F32),
            v((3, 2048, 128), BF16), v((4, 2, 64, 2048), BF16),
            v((4, 2, 16, 2048), BF16), v((4, 32, 2048), BF16),
            v((2, 128, 128), BF16), v((2, 128, 128), BF16),
            v((128, 128), BF16), v((3, 128, 128), BF16), v((4, 256, 128), BF16),
            v((4, 4, 256, 128), BF16), v((4, HEAD_DIM, 1024), BF16),
            v((4, 32, 8, 768), F32), v((4, 16, 8, 768), F32), v((4, 16, 16, 768), BF16),
            v((4, 4, HEAD_DIM, 256), F32), v((4, 4, 8, 256), F32),
            v((3, HEAD_DIM, 256), BF16), v((3, 1, 256), F32),
            v((3, HEAD_DIM, 256), BF16), v((3, 1, 256), F32),
            v((HEAD_DIM, 256), F32), v((8, 256), F32),
            v((8, 32, 128), BF16), v((8, 32, 128), BF16),
            dma((5,)), dma, dma((2, 3)), dma((2, 2)), dma, dma, dma, dma((3,)),
            dma, dma((3,)), dma, dma((2, 4)), dma((4,)),
            dma, dma((3,)), dma, dma((3,)),
            dma, dma, dma, dma, dma, dma, pltpu.SemaphoreType.REGULAR((3,)),
        ],
        compiler_params=pltpu.CompilerParams(has_side_effects=True, collective_id=0, vmem_limit_bytes=67043328),
    )(
        tokens.reshape(2, 16, 2048), norm_gain.reshape(1, 2048), score_offset,
        w_query, w_key, w_value, w_out.reshape(2, 64, 2048),
    )


def solution(mesh):
    rows = P(("sp", "tp"), None)
    placed = (rows, P(), P(None, "tp"), P(None, "tp"), P(None, "tp"), P("tp"), P("tp", None))
    return jax.shard_map(per_device, mesh=mesh, in_specs=placed, out_specs=rows, check_vma=False)
```

```python
import functools

import jax
import jax.numpy as jnp
from jax import lax
from jax.experimental import pallas as pl
from jax.experimental.pallas import tpu as pltpu
from jax.sharding import PartitionSpec as P

HEAD_DIM = 64
RMS_EPS = 1e-06
LOG2E = 1.4426950408889634
MESH = pl.DeviceIdType.MESH
NT = (((1,), (1,)), ((), ()))
NEG = -1e30
F32 = jnp.float32
BF16 = jnp.bfloat16


def dot(a, b):
    return jnp.dot(a, b, preferred_element_type=F32)


def layer_kernel(
    tok_hbm, gain_hbm, off_hbm, wq_hbm, wk_hbm, wv_hbm, wo_hbm, out_ref,
    tok_ref, gain_ref, off_ref, w_qkv, wo_all, tok_all, normed, sib_out, sib_in, q_out, q_in, q_pad,
    kv_all, vt_all, e_s, l_s, w_s, part_o, part_s, o_out, s_out, o_in, s_in, acc_o, acc_s,
    att_out, att_in,
    sem_w, ysend, yrecv, y2recv, bsend, brecv, qsend, qrecv,
    zsend, zrecv, xsend, xrecv, x2recv, osend, orecv, ssend, srecv,
    wsend, wrecv, w2send, w2recv, asend, arecv, hello,
):
    sp = lax.axis_index("sp")
    y = lax.axis_index("tp")
    z = sp // 8
    x = (sp // 2) % 4
    c = sp % 2
    group = z // 4
    r = z % 4

    def at(z_, x_, c_, y_):
        return ((z_ * 4 + x_) * 2 + c_, y_)

    def remote(src, dst, ss, rs, dev):
        return pltpu.make_async_remote_copy(
            src_ref=src, dst_ref=dst, send_sem=ss, recv_sem=rs, device_id=dev, device_id_type=MESH
        )

    def settle(ref, sem):
        pltpu.make_async_copy(ref, ref, sem).wait()

    early = [
        pltpu.make_async_copy(tok_hbm, tok_ref, sem_w.at[2]),
        pltpu.make_async_copy(gain_hbm, gain_ref, sem_w.at[3]),
        pltpu.make_async_copy(off_hbm, off_ref, sem_w.at[4]),
    ]
    for cp in early:
        cp.start()
    loads = [
        pltpu.make_async_copy(wq_hbm, w_qkv.at[0], sem_w.at[0]),
        pltpu.make_async_copy(wk_hbm, w_qkv.at[1], sem_w.at[0]),
        pltpu.make_async_copy(wv_hbm, w_qkv.at[2], sem_w.at[0]),
        pltpu.make_async_copy(wo_hbm, wo_all.at[y], sem_w.at[1]),
    ]
    for cp in loads:
        cp.start()

    y_up, y_dn, y_far = (y + 1) % 4, (y + 3) % 4, (y + 2) % 4
    peers = (at(z, x, c, y_up), at(z, x, c, y_dn))

    partner = at(z, x, 1 - c, y)
    sides = [at(z, (x + 1) % 4, c, y), at(z, (x + 3) % 4, c, y)]
    below = {1: (z + 12) % 16, 2: (z + 27 - 2 * r) % 16, 3: (z + 4) % 16}
    above = {1: (z + 4) % 16, 2: (z + 27 - 2 * r) % 16, 3: (z + 12) % 16}

    def tell(sem, dev):
        pl.semaphore_signal(sem, inc=1, device_id=dev, device_id_type=MESH)

    def greet(sem, devs, step):
        for dev in devs:
            tell(sem, dev)

        @pl.when(z >= step)
        def _():
            tell(sem, at(z - step, x, c, y))

        @pl.when(z + step <= 15)
        def _():
            tell(sem, at(z + step, x, c, y))

        return len(devs) + jnp.where(z >= step, 1, 0) + jnp.where(z + step <= 15, 1, 0)

    barrier = pltpu.get_barrier_semaphore()
    count = greet(barrier, [*peers, partner, *sides], 1)

    @pl.when(group == 0)
    def _():
        tell(barrier, at(above[3], x, c, y))

    @pl.when(jnp.logical_and(group < 2, r < 2))
    def _():
        tell(barrier, at(above[2], x, c, y))

    count = count + jnp.where(group == 3, 1, 0) + jnp.where(jnp.logical_and(group >= 2, r >= 2), 1, 0)
    pl.semaphore_wait(barrier, count)
    for cp in early:
        cp.wait()
    cols = (pl.ds(0, 1024), pl.ds(1024, 1024))
    first = {}
    for n in range(2):
        for d in range(2):
            first[d, n] = remote(
                tok_ref.at[d, :, cols[n]], tok_all.at[y, d, :, cols[n]], ysend, yrecv.at[d, n], peers[d]
            )
    for d in range(2):
        first[d, 2] = remote(tok_ref.at[1 - d], tok_all.at[y, 1 - d], ysend, yrecv.at[d, 2], peers[d])
    for cp in first.values():
        cp.start()

    pl.semaphore_wait(hello.at[0], greet(hello.at[0], [*peers, partner, *sides], 1))
    gain = gain_ref[...]

    def norm_rows(rows):
        rows = rows.astype(F32)
        inv = lax.rsqrt(jnp.mean(rows * rows, axis=1, keepdims=True) + RMS_EPS)
        return (rows * inv * gain).astype(BF16)

    for h in range(2):
        normed[y, pl.ds(h * 16, 16), :] = norm_rows(tok_ref[h])

    row_i = lax.broadcasted_iota(jnp.int32, (256, 256), 0)
    col_i = lax.broadcasted_iota(jnp.int32, (256, 256), 1)
    perm = jnp.where((row_i % 8) * 32 + row_i // 8 == col_i, 1.0, 0.0).astype(BF16)

    relays = []
    for n in range(2):
        for d in range(2):
            first[d, n].wait_recv()
            piece = tok_all.at[(y_dn, y_up)[d], d, :, cols[n]]
            relays.append(remote(piece, piece, ysend, y2recv.at[d, n], peers[d]))
            relays[-1].start()
    pl.semaphore_wait(hello.at[1], greet(hello.at[1], [partner], 2))
    told = greet(hello.at[2], [], 4)
    q_pad[...] = jnp.zeros((4, 256, 128), BF16)
    normed[y_dn, pl.ds(0, 16), :] = norm_rows(tok_all[y_dn, 0])
    normed[y_up, pl.ds(16, 16), :] = norm_rows(tok_all[y_up, 1])
    first[0, 2].wait_recv()
    normed[y_dn, pl.ds(16, 16), :] = norm_rows(tok_all[y_dn, 1])
    first[1, 2].wait_recv()
    normed[y_up, pl.ds(0, 16), :] = norm_rows(tok_all[y_up, 0])
    settle(w_qkv, sem_w.at[0])
    loads[3].wait()
    for d in range(2):
        relays[d].wait_recv()
        relays[d + 2].wait_recv()
        normed[y_far, pl.ds(16 * d, 16), :] = norm_rows(tok_all[y_far, d])

    rows = normed[...].reshape(128, 2048)
    q = dot(rows, w_qkv[0])
    k = dot(rows, w_qkv[1])
    v = dot(rows, w_qkv[2])
    lane = lax.broadcasted_iota(jnp.int32, (128, 128), 1)
    low = lane < HEAD_DIM
    kv0 = jnp.where(low, k, pltpu.roll(v, HEAD_DIM, 1)).astype(BF16)
    kv1 = jnp.where(low, pltpu.roll(k, HEAD_DIM, 1), v).astype(BF16)
    mine0 = c == 0
    sib_out[0] = jnp.where(mine0, kv1, kv0)
    sib_out[1] = pltpu.roll(q, HEAD_DIM, 1).astype(BF16)
    sib = remote(sib_out, sib_in, bsend, brecv, at(z, x, 1 - c, y))
    sib.start()
    kv_mine = jnp.where(mine0, kv0, kv1)

    for yy in (y_up, y_dn, y_far):
        remote(wo_all.at[y, c], wo_all.at[y, c], wsend, wrecv, at(z, x, c, yy)).start()
    three_halves = wo_all.at[pl.ds(0, 3), 0]

    sib.wait_recv()
    q_first = (lane < HEAD_DIM) == mine0
    q_out[...] = jnp.where(q_first, q, sib_in[1].astype(F32)).astype(BF16)
    kv_sib = sib_in[0]
    pair = jnp.concatenate([jnp.where(mine0, kv_mine, kv_sib), jnp.where(mine0, kv_sib, kv_mine)], axis=0)
    kv_all[r, x] = dot(perm, pair).astype(BF16)

    def q_copy(n):
        return remote(q_out, q_in.at[n - 1], qsend, qrecv.at[n - 1], at(below[n], x, c, y))

    planes = (r, r + 1 - 2 * (r % 2), (r + 2) % 4, 3 - r)

    def z_copy(n):
        return remote(
            kv_all.at[r, x], kv_all.at[r, x], zsend, zrecv.at[n - 1], at(group * 4 + planes[n], x, c, y)
        )

    def x_copy(d, n):
        block = kv_all.at[planes[n], x]
        return remote(block, block, xsend, xrecv.at[d, n], sides[d])

    def x_relay(n):
        if n < 2:
            block = kv_all.at[planes[n], (x + (3, 1)[n]) % 4]
            return remote(block, block, xsend, x2recv.at[n], sides[n])
        block = kv_all.at[planes[n], x]
        return remote(block, block, xsend, x2recv.at[n], at(z, (x + 2) % 4, c, y))

    def spread(n):
        if n:
            z_copy(n).wait_recv()
        x_copy(0, n).start()
        x_copy(1, n).start()
        if n >= 2:
            x_relay(n).start()

    def forward(n):
        x_copy(n, n).wait_recv()
        x_relay(n).start()

    low_half = lane < HEAD_DIM

    def complete(n):
        for d in range(2):
            if d != n:
                x_copy(d, n).wait_recv()
        x_relay(n).wait_recv()
        for b in range(4):
            vt_all[planes[n], :, pl.ds(b * 256, 256)] = (
                kv_all[planes[n], b].astype(F32).T[HEAD_DIM:, :].astype(BF16)
            )

    def pad_query(n, packed):
        packed = packed.astype(F32)
        q_pad[n, pl.ds(0, 128), :] = jnp.where(low_half, packed, 0.0).astype(BF16)
        q_pad[n, pl.ds(128, 128), :] = jnp.where(low_half, pltpu.roll(packed, HEAD_DIM, 1), 0.0).astype(BF16)

    def arrive(n):
        @pl.when(group + n <= 3)
        def _():
            q_copy(n).wait_recv()
            pad_query(n, q_in[n - 1])

    offset = off_ref[c] * LOG2E
    scale = HEAD_DIM ** (-0.5) * LOG2E
    ahead = lax.broadcasted_iota(jnp.int32, (8, 256), 0) * 32 - lax.broadcasted_iota(jnp.int32, (8, 256), 1)

    def block(*pairs):
        pairs = [(n, planes[m]) for n, m in pairs]
        wide = 256 * len(pairs)
        every = pl.ds(0, wide)
        sub = lax.broadcasted_iota(jnp.int32, (8, wide), 0)
        sums = []
        for b in range(4):
            total = [None] * len(pairs)
            for h, (n, plane) in enumerate(pairs):
                lanes = pl.ds(h * 256, 256)
                zz = lax.dot_general(kv_all[plane, b], q_pad[n], NT, preferred_element_type=F32)
                zz = zz.reshape(32, 8, 256)
                limit = x * 256 - b * 256 + (r - plane) * 1024
                for g in range(31, -1, -2):
                    up = []
                    for i in (g, g - 1):
                        e = jnp.exp2(jnp.minimum(zz[i] * scale + offset, 60.0))
                        if n == 0:
                            e = jnp.where(ahead < limit - i, e, 0.0)
                        e_s[b, i, :, lanes] = e
                        up.append(1.0 + e)
                    keep = jnp.log2(up[0] * up[1])
                    l_s[b, g // 2, :, lanes] = keep
                    total[h] = keep if total[h] is None else total[h] + keep
            sums.append(jnp.concatenate(total, axis=1))
        later = jnp.zeros((1, wide), F32)
        for b in range(3, -1, -1):
            total = sums[b]
            incl = total
            for step in (1, 2, 4):
                moved = pltpu.roll(incl, 8 - step, 0)
                incl = incl + jnp.where(sub < 8 - step, moved, 0.0)
            run = incl - total + later
            later = later + incl[0:1]
            for g in range(31, -1, -2):
                run = run + l_s[b, g // 2, :, every]
                left = jnp.exp2(-run)
                e = e_s[b, g - 1, :, every]
                w_s[b, g // 2, :, every] = jnp.concatenate(
                    [e * left, e_s[b, g, :, every] * (left * (1.0 + e))], axis=0
                ).astype(BF16)
        for h, (n, plane) in enumerate(pairs):
            part_o[n, plane] = dot(vt_all[plane], w_s[:, :, :, pl.ds(h * 256, 256)].reshape(1024, 256))
            part_s[n, plane] = jnp.broadcast_to(later[:, h * 256 : h * 256 + 256], (8, 256))

    for m in (1, 2, 3):
        @pl.when(planes[m] > r)
        def _():
            part_o[0, planes[m]] = jnp.zeros((HEAD_DIM, 256), F32)
            part_s[0, planes[m]] = jnp.zeros((8, 256), F32)

    def own_rest():
        for plane, pairs in ((1, ((0, 1),)), (2, ((0, 2), (0, 3))), (3, ((0, 1), (0, 2), (0, 3)))):
            @pl.when(r == plane)
            def _():
                block(*pairs)

    def near_groups(first, *pairs):
        @pl.when(jnp.logical_and(group >= first, group < 3))
        def _():
            block(*pairs)

    def group_is(g, *pairs):
        @pl.when(group == g)
        def _():
            block(*pairs)

    def two_groups(*pairs):
        @pl.when(group < 2)
        def _():
            block(*pairs)

    def finish(n):
        o = part_o[n, 3]
        s = part_s[n, 3][0:1]
        for plane in (2, 1, 0):
            o = o + jnp.exp2(-s) * part_o[n, plane]
            s = s + part_s[n, plane][0:1]
        return o, s

    def o_copy(n):
        dev = at(above[n], x, c, y)
        return (
            remote(o_out.at[n - 1], o_in.at[n - 1], osend, orecv.at[n - 1], dev),
            remote(s_out.at[n - 1], s_in.at[n - 1], ssend, srecv.at[n - 1], dev),
        )

    def give_back(n):
        @pl.when(group + n <= 3)
        def _():
            o, s = finish(n)
            o_out[n - 1] = o.astype(BF16)
            s_out[n - 1] = s
            for cp in o_copy(n):
                cp.start()

    def ask(n):
        @pl.when(group >= n)
        def _():
            q_copy(n).start()

    spread(0)
    z_copy(1).start()
    z_copy(2).start()
    z_copy(3).start()
    pl.semaphore_wait(hello.at[2], told)
    ask(2)
    pad_query(0, q_out[...])
    forward(0)
    spread(1)
    ask(1)
    ask(3)
    spread(2)
    complete(0)
    forward(1)
    block((0, 0))
    spread(3)
    arrive(2)
    two_groups((2, 0))
    arrive(1)
    arrive(3)
    group_is(0, (1, 0), (3, 0))
    group_is(1, (1, 0))
    complete(1)
    group_is(0, (2, 1), (1, 1), (3, 1))
    group_is(1, (2, 1), (1, 1))
    group_is(2, (1, 0), (1, 1))
    complete(2)
    group_is(0, (2, 2), (1, 2), (3, 2))
    group_is(1, (2, 2), (1, 2))
    complete(3)
    two_groups((2, 3))
    give_back(2)
    group_is(0, (1, 3), (3, 3))
    give_back(3)
    group_is(1, (1, 3))
    group_is(2, (1, 2), (1, 3))
    give_back(1)
    own_rest()

    settle(three_halves, wrecv)
    for yy in (y_dn, y_up, y_far):
        remote(wo_all.at[yy, c], wo_all.at[yy, c], w2send, w2recv, partner).start()

    o, s = finish(0)
    acc_o[...] = o
    acc_s[...] = jnp.broadcast_to(s, (8, 256))
    for n in (1, 2, 3):
        @pl.when(group >= n)
        def _():
            for cp in o_copy(n):
                cp.wait_recv()
            s_ = acc_s[0:1, :]
            acc_o[...] += jnp.exp2(-s_) * o_in[n - 1].astype(F32)
            acc_s[...] = jnp.broadcast_to(s_ + s_in[n - 1], (8, 256))

    o = acc_o[...]
    both = jnp.concatenate([jnp.where(mine0, o, 0.0), jnp.where(mine0, 0.0, o)], axis=0)
    att_out[...] = both.T.astype(BF16).reshape(8, 32, 128)
    for n in range(1, 8):
        cc = (c + n // 4) % 2
        yy = (y + n) % 4
        remote(att_out.at[cc * 4 + yy], att_in.at[y * 2 + c], asend, arecv, at(z, x, cc, yy)).start()
    att_in[y * 2 + c] = att_out[c * 4 + y]
    settle(three_halves, w2recv)
    settle(att_in.at[pl.ds(0, 7)], arecv)
    total = jnp.zeros((32, 2048), F32)
    for yy in range(4):
        feats = (att_in[2 * yy].astype(F32) + att_in[2 * yy + 1].astype(F32)).astype(BF16)
        part = dot(feats, wo_all[yy].reshape(128, 2048))
        total = total + part.astype(BF16).astype(F32)
    out_ref[...] = total.astype(BF16)

    settle(tok_all.at[pl.ds(0, 3)], ysend)
    sib.wait_send()
    settle(three_halves, wsend)
    settle(three_halves, w2send)
    settle(att_out.at[pl.ds(0, 7)], asend)
    settle(kv_all.at[0, pl.ds(0, 3)], zsend)
    settle(kv_all.at[pl.ds(0, 3)], xsend)
    for n in (1, 2, 3):
        @pl.when(group == n)
        def _():
            settle(q_in.at[pl.ds(0, n)], qsend)

        @pl.when(3 - group == n)
        def _():
            settle(o_in.at[pl.ds(0, n)], osend)
            settle(s_in.at[pl.ds(0, n)], ssend)


def per_device(tokens, norm_gain, w_query, w_key, w_value, score_offset, w_out):
    hbm = pl.BlockSpec(memory_space=pl.ANY)
    dma = pltpu.SemaphoreType.DMA
    v = pltpu.VMEM
    return pl.pallas_call(
        layer_kernel,
        out_shape=jax.ShapeDtypeStruct((32, 2048), BF16),
        in_specs=[hbm] * 7,
        out_specs=pl.BlockSpec(memory_space=pltpu.VMEM),
        scratch_shapes=[
            v((2, 16, 2048), BF16), v((1, 2048), F32), pltpu.SMEM((2,), F32),
            v((3, 2048, 128), BF16), v((4, 2, 64, 2048), BF16),
            v((4, 2, 16, 2048), BF16), v((4, 32, 2048), BF16),
            v((2, 128, 128), BF16), v((2, 128, 128), BF16),
            v((128, 128), BF16), v((3, 128, 128), BF16), v((4, 256, 128), BF16),
            v((4, 4, 256, 128), BF16), v((4, HEAD_DIM, 1024), BF16),
            v((4, 32, 8, 768), F32), v((4, 16, 8, 768), F32), v((4, 16, 16, 768), BF16),
            v((4, 4, HEAD_DIM, 256), F32), v((4, 4, 8, 256), F32),
            v((3, HEAD_DIM, 256), BF16), v((3, 1, 256), F32),
            v((3, HEAD_DIM, 256), BF16), v((3, 1, 256), F32),
            v((HEAD_DIM, 256), F32), v((8, 256), F32),
            v((8, 32, 128), BF16), v((8, 32, 128), BF16),
            dma((5,)), dma, dma((2, 3)), dma((2, 2)), dma, dma, dma, dma((3,)),
            dma, dma((3,)), dma, dma((2, 4)), dma((4,)),
            dma, dma((3,)), dma, dma((3,)),
            dma, dma, dma, dma, dma, dma, pltpu.SemaphoreType.REGULAR((3,)),
        ],
        compiler_params=pltpu.CompilerParams(has_side_effects=True, collective_id=0, vmem_limit_bytes=67043328),
    )(
        tokens.reshape(2, 16, 2048), norm_gain.reshape(1, 2048), score_offset,
        w_query, w_key, w_value, w_out.reshape(2, 64, 2048),
    )


def solution(mesh):
    rows = P(("sp", "tp"), None)
    placed = (rows, P(), P(None, "tp"), P(None, "tp"), P(None, "tp"), P("tp"), P("tp", None))
    return jax.shard_map(per_device, mesh=mesh, in_specs=placed, out_specs=rows, check_vma=False)
```
